32 devices in a mesh: sp: 4 (over y, x), tp: 8 (over z, core).
Axes of the slice: x: 2, y: 2, z: 4, core: 2. Of those that a mesh axis runs over, the one named last changes fastest.
Arguments:
- mix_in: bfloat16 [4096, 2048], P('sp', 'tp'), may hold values from -8 to 8
- gate_in: bfloat16 [4096, 2048], P('sp', 'tp'), may hold values from -6 to 6
- conv_w: float32 [4, 2048], P(None, 'tp'), may hold values from -3 to 3
- conv_b: float32 [2048], P('tp'), may hold values from -3 to 3
- decay_param: float32 [2, 2048], P(None, 'tp')
- recur_gate: float32 [2, 32, 64, 64], P(None, 'tp'), may hold values from -0.75 to 0.75
- recur_bias: float32 [2, 2048], P(None, 'tp'), may hold values from -4 to 4
- input_gate: float32 [2, 32, 64, 64], P(None, 'tp'), may hold values from -0.75 to 0.75
- input_bias: float32 [2, 2048], P(None, 'tp'), may hold values from -4 to 4
- residual: bfloat16 [4096, 2048], P(('sp', 'tp')), may hold values from -6 to 6
- out_proj: bfloat16 [2048, 2048], replicated, may hold values from -0.125 to 0.125
- norm_gain: float32 [3, 2048], replicated, may hold values from 0.1 to 1.9
- routes: int32 [4096, 2], P('sp'), may hold values from 0 to 15, all different within a row; in each aligned block of 128 rows (0 to 127, 128 to 255, ...) at most 32 rows name the same one
- route_wt: float32 [4096, 2], P('sp'), may hold values from 0.1 to 1
- exp_gate: bfloat16 [16, 2048, 1024], P('sp', None, 'tp'), may hold values from -0.125 to 0.125
- exp_up: bfloat16 [16, 2048, 1024], P('sp', None, 'tp'), may hold values from -0.125 to 0.125
- exp_down: bfloat16 [16, 1024, 2048], P('sp', 'tp'), may hold values from -0.1875 to 0.1875
Outputs:
- final: bfloat16 [4096, 2048], P(('sp', 'tp'))
The draws below stay inside these ranges and needn't reach their ends.
Inputs may be any that keep to these rules, and one draw needn't show every extreme that they name: `routes`: in each aligned block of 128 tokens (the rows of one device in the expert layer) no expert is named more than 32 times, and in some block some expert exactly 32 times; a token's 2 experts differ.
All inputs are finite; a program needn't handle non-finite values.
Results may differ from the reference program's by a relative error of at most 0.008.
Values may be sent and summed in bfloat16 or wider, within the bound.
A program may use at most 128 MiB of HBM per device.

```python
import math
import jax
import jax.numpy as jnp
import numpy as np
from jax import lax

D = 2048
WIDTH = 2048
HEAD = 64
FF = 1024
EXPERTS = 16
TOPK = 2
SEQ_DEV = 1024
HEADS = 32
SEQ = 4096
ROWS = 128
CAP = 32


def draw_decay_param(key, part):
    pick_key, slow_key, fast_key = jax.random.split(jax.random.fold_in(key, 17), 3)
    slow_share = 0.5
    chooser = jax.random.uniform(pick_key, (2, WIDTH), jnp.float32)
    slow_values = math.log(SEQ) + jax.random.uniform(slow_key, (2, WIDTH), jnp.float32, 0.7, 1.7)
    fast_values = jax.random.uniform(fast_key, (2, WIDTH), jnp.float32, 3.5, 5.0)
    return jnp.where(chooser < slow_share, slow_values, fast_values).astype(jnp.float32)


def draw_conv_w(key, part):
    tap_key = jax.random.fold_in(key, 31)
    values = jax.random.normal(tap_key, (4, WIDTH), jnp.float32)
    tap_scale = jnp.array([0.4, 0.4, 0.4, 1.2], jnp.float32)[:, None]
    return jnp.clip(values * tap_scale, -3.0, 3.0).astype(jnp.float32)


def draw_mix_in(key, part):
    value_key, scale_key, offset_key = jax.random.split(jax.random.fold_in(key, 23), 3)
    values = jax.random.normal(value_key, (SEQ, WIDTH), jnp.float32)
    spread = 0.8
    position = jnp.arange(SEQ, dtype=jnp.int32) % SEQ_DEV
    at_ends = jnp.logical_or(position < 2, position >= SEQ_DEV - 2)
    values = values * jnp.where(at_ends, 3.0, 1.0)[:, None]
    scales = jnp.exp(jax.random.uniform(scale_key, (SEQ // 64, 1, WIDTH), jnp.float32, -spread, spread))
    shaped = (values.reshape(SEQ // 64, 64, WIDTH) * scales).reshape(SEQ, WIDTH)
    offsets = jax.random.uniform(offset_key, (SEQ // SEQ_DEV, 1, WIDTH), jnp.float32, -1.5, 1.5)
    shifted = (shaped.reshape(SEQ // SEQ_DEV, SEQ_DEV, WIDTH) + offsets).reshape(SEQ, WIDTH)
    return jnp.clip(shifted, -8.0, 8.0).astype(jnp.bfloat16)


def level_of(key, extent, shards, smallest, high):
    loudness, own = 1.0, jax.random.fold_in(key, 6)
    for dim, parts in shards:
        draws = jnp.exp(jax.random.uniform(jax.random.fold_in(own, dim), (parts,), jnp.float32, smallest / len(shards), high / len(shards)))
        loudness = loudness * jnp.repeat(draws, extent[dim] // parts).reshape([-1 if axis == dim else 1 for axis in range(len(extent))])
    return loudness


def deal_out(stream_key, own, number, rows, count, top, reach, lean):
    sequence = jax.random.permutation(stream_key, count)
    crowded, ordinary = load_shares(count, rows * top, reach, lean, True), load_shares(count, rows * top, reach, lean, False)
    places = jnp.arange(count)

    def named(tallies, rotation):
        used = int((tallies > 0).sum())
        fixed = max(1, used // 4)
        passed = fixed + (places - fixed + rotation * (used - fixed)) % max(1, count - fixed)
        return jnp.zeros((count,), jnp.int32).at[sequence[jnp.where(places < fixed, places, passed)]].set(jnp.asarray(tallies, jnp.int32))

    tallies = jnp.where(number % 4 == 0, named(crowded, number // 4), named(ordinary, number - number // 4 - 1))
    mixed = jax.random.permutation(jax.random.fold_in(own, 3), count)
    source_of, sink = mixed[0:count // 2 * 2:2], mixed[1:count // 2 * 2:2]
    room = jnp.minimum(tallies[source_of] - 1, reach - tallies[sink]) // 2
    room = jnp.where((source_of == sequence[0]) | (sink == sequence[0]) | (tallies[sink] == 0), 0, jnp.maximum(room, 0))
    passed = jax.random.randint(jax.random.fold_in(own, 4), (count // 2,), 0, 1 << 20) % (room + 1)
    tallies = tallies.at[source_of].add(-passed).at[sink].add(passed)
    items = jnp.searchsorted(jnp.cumsum(tallies), jnp.arange(rows * top), side="right").astype(jnp.int32)
    table = items.reshape(top, rows).T
    table = table[jax.random.permutation(jax.random.fold_in(own, 1), rows)]
    rotation = jax.random.randint(jax.random.fold_in(own, 2), (rows, 1), 0, top)
    return jnp.take_along_axis(table, (jnp.arange(top)[None, :] + rotation) % top, axis=1)


def load_shares(count, total, most, lean, full):
    portions = [(1 << 20) // math.isqrt(standing ** lean) + 1 for standing in range(1, count + 1)]
    largest = most if full else min(most, max(-(-total // count), total * portions[0] // sum(portions)))
    least = 1 if total - largest >= count - 1 else 0
    holding, surplus = [largest] + [least] * (count - 1), total - largest - least * (count - 1)
    while surplus > 0:
        movable = [i for i in range(1, count) if holding[i] < largest] or [i for i in range(1, count) if holding[i] < most]
        pool, budget = sum([portions[i] for i in movable]), surplus
        for i in movable:
            more = min(most - holding[i], max(1, budget * portions[i] // pool), surplus)
            holding[i] = holding[i] + more
            surplus = surplus - more
    return np.array(holding)


def centred(stream_key, dims, deviation, limit, cuts=(), held_as=jnp.bfloat16):
    entries = jax.random.normal(stream_key, dims, jnp.float32) * deviation
    if len(cuts) > 0:
        entries = level_of(stream_key, dims, cuts, -0.22, 0.18) * entries
    return jnp.clip(entries, min=-limit, max=limit).astype(held_as)


def setup_inputs(seed: int = 0) -> dict:
    splits = jax.random.split(jax.random.key(seed), 18)
    mix_in = draw_mix_in(jax.random.fold_in(splits[17], 71), 0)
    gate_in = centred(splits[1], (SEQ, WIDTH), 1.0, 6.0, ((0, 4), (1, 8)))
    conv_w = draw_conv_w(jax.random.fold_in(splits[17], 71), 0)
    conv_b = centred(splits[3], (WIDTH,), 0.5, 3.0, ((0, 8),), jnp.float32)
    decay_param = draw_decay_param(jax.random.fold_in(splits[17], 71), 0)
    recur_gate = centred(splits[5], (2, HEADS, HEAD, HEAD), HEAD ** -0.5, 0.75, ((1, 8),), jnp.float32)
    recur_bias = centred(splits[6], (2, WIDTH), 1.0, 4.0, ((1, 8),), jnp.float32)
    input_gate = centred(splits[7], (2, HEADS, HEAD, HEAD), HEAD ** -0.5, 0.75, ((1, 8),), jnp.float32)
    input_bias = centred(splits[8], (2, WIDTH), 1.0, 4.0, ((1, 8),), jnp.float32)
    residual = centred(splits[9], (SEQ, D), 1.0, 6.0, ((0, 32),))
    out_proj = centred(splits[10], (WIDTH, D), WIDTH ** -0.5, 0.125)
    norm_gain = jnp.clip(1.0 + 0.18 * jax.random.normal(splits[11], (3, D), jnp.float32), 0.1, 1.9)
    routes_keys = jax.random.split(jax.random.fold_in(splits[12], 1), SEQ // ROWS)
    routes_turns = jax.random.permutation(jax.random.fold_in(splits[12], 3), SEQ // ROWS)
    routes = jax.vmap(lambda own, number: deal_out(jax.random.fold_in(splits[12], 2), own, number, ROWS, EXPERTS, TOPK, CAP, 2))(routes_keys, routes_turns).reshape((SEQ, TOPK))
    route_wt = jnp.clip(0.1 + 0.9 * jax.random.uniform(splits[13], (SEQ, TOPK), jnp.float32) ** level_of(splits[13], (SEQ, TOPK), ((0, 4),), -0.2, 0.2), 0.1, 1.0)
    exp_gate = centred(splits[14], (EXPERTS, D, FF), D ** -0.5, 0.125, ((0, 4), (2, 8)))
    exp_up = centred(splits[15], (EXPERTS, D, FF), D ** -0.5, 0.125, ((0, 4), (2, 8)))
    exp_down = centred(splits[16], (EXPERTS, FF, D), FF ** -0.5, 0.1875, ((0, 4), (1, 8)))
    return {"mix_in": mix_in, "gate_in": gate_in, "conv_w": conv_w, "conv_b": conv_b, "decay_param": decay_param, "recur_gate": recur_gate, "recur_bias": recur_bias, "input_gate": input_gate, "input_bias": input_bias, "residual": residual, "out_proj": out_proj, "norm_gain": norm_gain, "routes": routes, "route_wt": route_wt, "exp_gate": exp_gate, "exp_up": exp_up, "exp_down": exp_down}


EPSILON = 1e-06
HIGHEST_MODE = lax.Precision.HIGHEST

def norm_rows(values, gain):
    floats = values.astype(jnp.float32)
    return floats * lax.rsqrt(lax.optimization_barrier(jnp.mean(floats * floats, axis=-1, keepdims=True)) + EPSILON) * gain

def pair_join(earlier, later_pair):
    return (earlier[0] * later_pair[0], later_pair[0] * earlier[1] + later_pair[1])

def slot_table(route_rows, experts, capacity):
    row_count, top_count = route_rows.shape
    flattened = route_rows.reshape(row_count * top_count)
    matches = (flattened[:, None] == jnp.arange(experts, dtype=jnp.int32)[None, :]).astype(jnp.int32)
    earlier_hits = jnp.cumsum(matches, axis=0) - matches
    position = lax.optimization_barrier(jnp.sum(earlier_hits * matches, axis=1))
    return (flattened * capacity + position).reshape(row_count, top_count)

def coefficients(conv_out, recur_blocks, recur_bias, input_blocks, input_bias, decay_param):
    seq_len, channels = conv_out.shape
    heads, head_dim, _ = recur_blocks.shape
    blocked = conv_out.reshape(seq_len, heads, head_dim)
    recur_pre = jnp.einsum('lhi,hij->lhj', blocked, recur_blocks, precision=HIGHEST_MODE).reshape(seq_len, channels)
    input_pre = jnp.einsum('lhi,hij->lhj', blocked, input_blocks, precision=HIGHEST_MODE).reshape(seq_len, channels)
    recur_act = jax.nn.sigmoid(recur_pre + recur_bias)
    input_act = jax.nn.sigmoid(input_pre + input_bias)
    log_decay = -8.0 * recur_act * jax.nn.softplus(-decay_param)
    return (jnp.exp(log_decay), jnp.sqrt(-jnp.expm1(2.0 * log_decay)) * (input_act * conv_out))

def expert_apply(operands):
    tokens_in, gate_w, up_w, down_w = operands
    gate_act = jnp.dot(tokens_in, gate_w, preferred_element_type=jnp.float32)
    up_act = jnp.dot(tokens_in, up_w, preferred_element_type=jnp.float32)
    hidden = (jax.nn.silu(gate_act) * up_act).astype(jnp.bfloat16)
    return jnp.dot(hidden, down_w, preferred_element_type=jnp.float32).astype(jnp.bfloat16)

def reference(mix_in, gate_in, conv_w, conv_b, decay_param, recur_gate, recur_bias, input_gate, input_bias, residual, out_proj, norm_gain, routes, route_wt, exp_gate, exp_up, exp_down):
    seq_len = mix_in.shape[0]
    padded = jnp.pad(mix_in.astype(jnp.float32), ((2, 1), (0, 0)))
    conv_out = conv_b + padded[0:seq_len] * conv_w[0]
    for tap in range(1, conv_w.shape[0]):
        conv_out = conv_out + padded[tap:tap + seq_len] * conv_w[tap]
    state_sum = jnp.zeros_like(conv_out)
    for sense in range(2):
        decay, drive = coefficients(conv_out, recur_gate[sense], recur_bias[sense], input_gate[sense], input_bias[sense], decay_param[sense])
        if sense == 1:
            decay, drive = (jnp.flip(decay, 0), jnp.flip(drive, 0))
        _, states = lax.associative_scan(pair_join, (decay, drive), axis=0)
        if sense == 1:
            states = jnp.flip(states, 0)
        state_sum = state_sum + states
    mixed = (state_sum * jax.nn.gelu(gate_in.astype(jnp.float32))).astype(jnp.bfloat16)
    proj = jnp.dot(mixed, out_proj, preferred_element_type=jnp.float32).astype(jnp.bfloat16)
    proj = lax.optimization_barrier(proj)
    stream = (residual.astype(jnp.float32) + norm_rows(proj, norm_gain[0])).astype(jnp.bfloat16)
    stream = lax.optimization_barrier(stream)
    normed = norm_rows(stream, norm_gain[1]).astype(jnp.bfloat16)
    nblocks = seq_len // ROWS
    route_blocks = routes.reshape(nblocks, ROWS, TOPK)
    slots = jax.vmap(lambda block: slot_table(block, EXPERTS, CAP))(route_blocks)
    source_rows = jnp.repeat(jnp.arange(ROWS, dtype=jnp.int32), TOPK)

    def fill_table(slot_rows):
        empty = jnp.full((EXPERTS * CAP,), ROWS, jnp.int32)
        return empty.at[slot_rows.reshape(ROWS * TOPK)].set(source_rows)
    table = jax.vmap(fill_table)(slots)
    blocks_pad = jnp.concatenate([normed.reshape(nblocks, ROWS, D), jnp.zeros((nblocks, 1, D), jnp.bfloat16)], axis=1)
    dispatched = jnp.take_along_axis(blocks_pad, table[:, :, None], axis=1)
    by_expert = jnp.moveaxis(dispatched.reshape(nblocks, EXPERTS, CAP, D), 1, 0).reshape(EXPERTS, nblocks * CAP, D)
    results = lax.map(expert_apply, (by_expert, exp_gate, exp_up, exp_down)).reshape(EXPERTS, nblocks, CAP, D)
    slot_place = (slots % CAP).astype(jnp.int32)
    expert_ids = (slots // CAP).astype(jnp.int32)
    block_ids = jnp.arange(nblocks, dtype=jnp.int32)[:, None, None]
    picked = results[expert_ids, block_ids, slot_place]
    weights = route_wt.reshape(nblocks, ROWS, TOPK)[..., None]
    mixture = lax.optimization_barrier(jnp.sum(weights * picked.astype(jnp.float32), axis=2)).reshape(seq_len, D).astype(jnp.bfloat16)
    mixture = lax.optimization_barrier(mixture)
    return (stream.astype(jnp.float32) + norm_rows(mixture, norm_gain[2])).astype(jnp.bfloat16)
```

```python
import functools

import jax
import jax.numpy as jnp
from jax import lax
from jax.experimental import pallas as pl
from jax.experimental.pallas import tpu as pltpu
from jax.sharding import PartitionSpec as P

EPSILON = 1e-06
HIGHEST_MODE = lax.Precision.HIGHEST
MESH = pl.DeviceIdType.MESH
HALO = 16
SUB = 8
LAG = 2
RING = 2


def norm_rows(values, gain):
    floats = values.astype(jnp.float32)
    return floats * lax.rsqrt(jnp.mean(floats * floats, axis=-1, keepdims=True) + EPSILON) * gain


def slot_tables(routes, route_wt, dims, rows, cap, local):
    S, T, L, Z = dims
    top = routes.shape[1]
    pair = 2 * rows
    flat = routes.reshape(T, rows * top).T
    wanted = jnp.arange(S, dtype=jnp.int32) * L + local
    matches = flat[:, :, None] == wanted
    order = jnp.arange(rows * top, dtype=jnp.int32)
    before = (order[None, :] < order[:, None]).astype(jnp.bfloat16)
    earlier = jnp.dot(
        before, matches.reshape(rows * top, T * S).astype(jnp.bfloat16),
        preferred_element_type=jnp.float32,
    ).reshape(rows * top, T, S)
    core = (jnp.arange(T, dtype=jnp.int32) % 2)[:, None]
    slot = (jnp.arange(S, dtype=jnp.int32) * 2 + core) * cap
    ids = jnp.where(matches, earlier.astype(jnp.int32) + slot + 1, 0).sum(axis=2) - 1
    ids = ids.reshape(rows, top, T)
    by_slot = ids.transpose(2, 0, 1).reshape(Z, pair, top)
    weights = route_wt.reshape(Z, pair, top)
    return by_slot.transpose(0, 2, 1), by_slot, weights


def one_minus_exp(y):
    series = -y * (1.0 + y * (1.0 / 2) * (1.0 + y * (1.0 / 3) * (1.0 + y * 0.25 * (1.0 + y * 0.2))))
    return jnp.where(y > -0.1, series, 1.0 - jnp.exp(y))


def split_f32(x):
    high = x.astype(jnp.bfloat16)
    return high, (x - high.astype(jnp.float32)).astype(jnp.bfloat16)


def tile_scan(a, b, reverse):
    row = lax.broadcasted_iota(jnp.int32, a.shape, 1)
    step = 1
    while step < SUB:
        shift = SUB - step if reverse else step
        keep = row < SUB - step if reverse else row >= step
        a_prev = jnp.where(keep, pltpu.roll(a, shift, 1), 1.0)
        b_prev = jnp.where(keep, pltpu.roll(b, shift, 1), 0.0)
        b = b + a * b_prev
        a = a * a_prev
        step *= 2
    return a, b


def layer_kernel(
    dims,
    mix_ref, gate_ref, cw_ref, cb_ref, soft_ref, rg_ref, rb_ref, ig_ref, ib_ref,
    res_ref, gain_ref, sel_ref, comb_ref, wt_ref, op_hbm, eg_hbm, eu_hbm, ed_hbm,
    out_ref,
    xp, wh, wl, af, bf, ab, bb, mixed, tok, op, proj, halo, summ, ends,
    wg, wu, wd, hid, stream, gath, outg, arr, back, prem, zrec, pbuf,
    op_sem, own_sem, halo_send, halo_recv, sum_send, sum_recv,
    mix_send, mix_recv, w_send, w_recv, ga_send, ga_recv, d2_send, d2_recv,
    dis_send, dis_recv, ret_send, ret_recv, pd_send, pd_recv, zs_send, zs_recv,
):
    S, T, L, Z = dims
    seq, C = mix_ref.shape
    rows, D = res_ref.shape
    two_cap = arr.shape[2]
    slots = S * two_cap
    heads, hd = rg_ref.shape[1], rg_ref.shape[2]
    F = eg_hbm.shape[2]
    sp = lax.axis_index("sp")
    tp = lax.axis_index("tp")
    z = lax.div(tp, 2)
    g = lax.rem(tp, 2)
    local = lax.rem(tp, L)
    part_base = tp - local
    partner = tp + 1 - 2 * g

    op_copy = pltpu.make_async_copy(op_hbm, op, op_sem)
    op_copy.start()

    barrier = pltpu.get_barrier_semaphore()
    greeted = 0
    for ds in range(S):
        for dt in range(T):
            if (ds == 0) != (dt == 0):
                pl.semaphore_signal(
                    barrier, inc=1,
                    device_id=(lax.rem(sp + ds, S), lax.rem(tp + dt, T)),
                    device_id_type=MESH,
                )
                greeted += 1
    pl.semaphore_wait(barrier, greeted)

    def remote(src, dst, send, recv, sp_to, tp_to):
        return pltpu.make_async_remote_copy(
            src_ref=src, dst_ref=dst, send_sem=send, recv_sem=recv,
            device_id=(sp_to, tp_to), device_id_type=MESH,
        )

    to_next = remote(mix_ref.at[pl.ds(seq - HALO, HALO)], halo.at[0], halo_send.at[0],
                     halo_recv.at[0], lax.rem(sp + 1, S), tp)
    to_prev = remote(mix_ref.at[pl.ds(0, HALO)], halo.at[1], halo_send.at[1],
                     halo_recv.at[1], lax.rem(sp + S - 1, S), tp)
    to_next.start()
    to_prev.start()

    tensors = ((eg_hbm, wg, 1), (eu_hbm, wu, 1), (ed_hbm, wd, 0))

    def chunk(ref, axis, place):
        if len(ref.shape) == 3:
            return ref.at[place]
        if ref.shape[axis] == F:
            return ref
        start = pl.multiple_of(place * F, F)
        return ref.at[:, pl.ds(start, F)] if axis else ref.at[pl.ds(start, F), :]

    def weight_copy(i, d):
        src, dst, axis = tensors[i]
        to = lax.rem(local + d, L)
        return remote(src.at[to], chunk(dst, axis, local), w_send.at[d - 1, i],
                      w_recv.at[d - 1, i], sp, part_base + to)

    own_weights = [
        pltpu.make_async_copy(src.at[local], chunk(dst, axis, local), own_sem.at[i])
        for i, (src, dst, axis) in enumerate(tensors)
    ]
    for c in own_weights:
        c.start()
    for i in range(2):
        for d in range(1, L):
            weight_copy(i, d).start()

    wh[...] = jnp.zeros_like(wh)
    wl[...] = jnp.zeros_like(wl)
    for k, ref in enumerate((rg_ref, ig_ref)):
        for sense in range(2):
            for h in range(heads):
                high, low = split_f32(ref[sense, h])
                col = (2 * sense + k) * C + h * hd
                wh[h * hd : (h + 1) * hd, col : col + hd] = high
                wl[h * hd : (h + 1) * hd, col : col + hd] = low
    xp[SUB : SUB + seq, :] = mix_ref[...].astype(jnp.float32)
    to_next.wait()
    to_prev.wait()
    tail = halo[0].astype(jnp.float32)[HALO - SUB : HALO]
    head = halo[1].astype(jnp.float32)[0:SUB]
    xp[0:SUB, :] = jnp.where(sp > 0, tail, 0.0)
    xp[SUB + seq : 2 * SUB + seq, :] = jnp.where(sp < S - 1, head, 0.0)

    R = min(128, seq)

    def gates(n, _):
        base = pl.multiple_of(n * R, R)
        window = xp[pl.ds(base, R + 2 * SUB), :]
        conv = cb_ref[...] + window[SUB - 2 : SUB - 2 + R] * cw_ref[0:1]
        for tap in range(1, cw_ref.shape[0]):
            conv = conv + window[SUB - 2 + tap : SUB - 2 + tap + R] * cw_ref[tap : tap + 1]
        high, low = split_f32(conv)
        for sense, (a_ref, b_ref) in enumerate(((af, bf), (ab, bb))):
            cols = slice(2 * sense * C, (2 * sense + 2) * C)
            pre = jnp.dot(high, wh[:, cols], preferred_element_type=jnp.float32)
            pre = pre + jnp.dot(low, wh[:, cols], preferred_element_type=jnp.float32)
            pre = pre + jnp.dot(high, wl[:, cols], preferred_element_type=jnp.float32)
            recur = jax.nn.sigmoid(pre[:, :C] + rb_ref[sense : sense + 1])
            inp = jax.nn.sigmoid(pre[:, C:] + ib_ref[sense : sense + 1])
            log_a = -8.0 * recur * soft_ref[sense : sense + 1]
            a = jnp.exp(log_a)
            b = jnp.sqrt(one_minus_exp(2.0 * log_a)) * (inp * conv)
            a, b = tile_scan(
                a.reshape(R // SUB, SUB, C), b.reshape(R // SUB, SUB, C), sense == 1
            )
            a_ref[pl.ds(base, R), :] = a.reshape(R, C)
            b_ref[pl.ds(base, R), :] = b.reshape(R, C)
        return 0

    lax.fori_loop(0, seq // R, gates, 0)

    tiles = seq // SUB

    def carry(t, held):
        sf, pf, sb, pb = held
        at = pl.ds(pl.multiple_of(t * SUB, SUB), SUB)
        a = af[at, :]
        s = bf[at, :] + a * sf
        p = a * pf
        af[at, :] = p
        bf[at, :] = s
        back = pl.ds(pl.multiple_of((tiles - 1 - t) * SUB, SUB), SUB)
        a = ab[back, :]
        s2 = bb[back, :] + a * sb
        p2 = a * pb
        ab[back, :] = p2
        bb[back, :] = s2
        return s[SUB - 1 : SUB], p[SUB - 1 : SUB], s2[0:1], p2[0:1]

    zero, one = jnp.zeros((1, C), jnp.float32), jnp.ones((1, C), jnp.float32)
    sf, pf, sb, pb = lax.fori_loop(0, tiles, carry, (zero, one, zero, one), unroll=4)
    summ[0:1, :] = sf
    summ[1:2, :] = pf
    summ[2:3, :] = sb
    summ[3:4, :] = pb
    sums = [
        remote(summ, ends.at[ds - 1], sum_send.at[ds - 1], sum_recv.at[ds - 1],
               lax.rem(sp + ds, S), tp)
        for ds in range(1, S)
    ]
    for c in sums:
        c.start()
    for c in sums:
        c.wait()
    fe, be = zero, zero
    for ds in range(S - 1, 0, -1):
        fe = jnp.where(sp >= ds, ends[ds - 1, 1:2, :] * fe + ends[ds - 1, 0:1, :], fe)
    for ds in range(1, S):
        be = jnp.where(sp + S - ds < S, ends[ds - 1, 3:4, :] * be + ends[ds - 1, 2:3, :], be)

    def join(n, _):
        at = pl.ds(pl.multiple_of(n * R, R), R)
        state = (bf[at, :] + af[at, :] * fe) + (bb[at, :] + ab[at, :] * be)
        mixed[at, :] = (state * jax.nn.gelu(gate_ref[at, :].astype(jnp.float32))).astype(
            jnp.bfloat16
        )
        return 0

    lax.fori_loop(0, seq // R, join, 0)

    def block_rows(place):
        return mixed.at[pl.ds(pl.multiple_of(place * rows, rows), rows), :]

    columns = pl.ds(pl.multiple_of(tp * C, C), C)
    moves = []
    for dt in range(1, T):
        to = lax.rem(tp + dt, T)
        moves.append(remote(block_rows(to), tok.at[:, columns], mix_send.at[dt],
                            mix_recv.at[dt], sp, to))
    for c in moves:
        c.start()
    own_move = pltpu.make_async_copy(block_rows(tp), tok.at[:, columns], own_sem.at[6])
    own_move.start()
    op_copy.wait()
    own_move.wait()
    for c in moves:
        c.wait()

    def project(n, _):
        cols = pl.ds(pl.multiple_of(n * 256, 256), 256)
        proj[:, cols] = (
            jnp.dot(tok[...], op[:, cols], preferred_element_type=jnp.float32)
            .astype(jnp.bfloat16)
        )
        return 0

    lax.fori_loop(0, D // 256, project, 0)
    part = 32

    def norms(n, _):
        at = pl.ds(pl.multiple_of(n * part, part), part)
        s = (
            res_ref[at, :].astype(jnp.float32) + norm_rows(proj[at, :], gain_ref[0:1, :])
        ).astype(jnp.bfloat16)
        stream[at, :] = s
        gath[tp, at, :] = norm_rows(s, gain_ref[1:2, :]).astype(jnp.bfloat16)
        return 0

    lax.fori_loop(0, rows // part, norms, 0)
    wide = min(256, D)

    def chip_at(j):
        low = jnp.minimum(z, Z - 1 - z)
        d = lax.div(j + 1, 2)
        near = jnp.where(lax.rem(j, 2) == 1, z - d, z + d)
        far = jnp.where(z < Z - 1 - z, j, Z - 1 - j)
        return jnp.where(j <= 2 * low, near, far)

    def along(zc, way):
        block = gath.at[2 * zc + g]
        return remote(block, block, ga_send.at[way, zc], ga_recv.at[zc], sp, tp + 2 - 4 * way)

    def across(zc):
        block = gath.at[2 * zc + g]
        return remote(block, block, d2_send.at[zc], d2_recv.at[zc], sp, partner)

    ring = outg.shape[0]

    def dispatch(j, ds):
        zc = chip_at(j)
        to = lax.rem(sp + ds, S)
        return remote(outg.at[lax.rem(j, ring), to], arr.at[zc, sp], dis_send.at[zc, ds - 1],
                      dis_recv.at[zc, ds - 1], to, tp)

    def give_back(zc, ds):
        to = lax.rem(sp + ds, S)
        return remote(arr.at[zc, to], back.at[zc, sp], ret_send.at[zc, ds - 1],
                      ret_recv.at[zc, ds - 1], to, tp)

    def merge(zc):
        return remote(gath.at[2 * zc + 1 - g], prem.at[zc], pd_send.at[zc], pd_recv.at[zc],
                      sp, partner)

    def deliver(zc):
        return remote(gath.at[2 * zc + g], zrec.at[z], zs_send.at[zc], zs_recv.at[z],
                      sp, 2 * zc + g)

    def gather_step(j):
        zc = chip_at(j)

        @pl.when(j > 0)
        def _():
            pltpu.make_async_copy(gath.at[2 * zc + g], gath.at[2 * zc + g], ga_recv.at[zc]).wait()

        across(zc).start()

        @pl.when((zc <= z) & (z < Z - 1))
        def _():
            along(zc, 0).start()

        @pl.when((zc >= z) & (z > 0))
        def _():
            along(zc, 1).start()

        @pl.when(j == min(1, Z - 1))
        def _():
            for d in range(1, L):
                weight_copy(2, d).start()

        across(zc).wait_recv()
        slot_id = lax.broadcasted_iota(jnp.int32, (slots, 2 * rows), 0)
        hit = slot_id == sel_ref[zc, 0:1, :]
        for k in range(1, sel_ref.shape[1]):
            hit = hit | (slot_id == sel_ref[zc, k : k + 1, :])
        selector = jnp.where(hit, 1.0, 0.0).astype(jnp.bfloat16)
        slot = lax.rem(j, ring)

        @pl.when(j >= ring)
        def _():
            for ds in range(1, S):
                dispatch(j - ring, ds).wait_send()

        def pick(n, _):
            cols = pl.ds(pl.multiple_of(n * wide, wide), wide)
            tokens = gath[pl.ds(2 * zc, 2), :, cols].reshape(2 * rows, wide)
            picked = jnp.dot(selector, tokens, preferred_element_type=jnp.float32)
            outg[slot, :, :, cols] = picked.astype(jnp.bfloat16).reshape(S, two_cap, wide)
            return 0

        lax.fori_loop(0, D // wide, pick, 0)
        for ds in range(1, S):
            dispatch(j, ds).start()
        arr[zc, sp] = outg[slot, sp]

    def expert_step(j):
        zc = chip_at(j)

        @pl.when(j == 0)
        def _():
            for c in own_weights:
                c.wait()
            for i in range(3):
                for d in range(1, L):
                    weight_copy(i, d).wait_recv()

        for ds in range(1, S):
            dispatch(j, ds).wait_recv()

        def activate(x, gate_w, up_w):
            gate_act = jnp.dot(x, gate_w, preferred_element_type=jnp.float32)
            up_act = jnp.dot(x, up_w, preferred_element_type=jnp.float32)
            return (jax.nn.silu(gate_act) * up_act).astype(jnp.bfloat16)

        x = arr[zc].reshape(slots, D)
        if len(wg.shape) == 3:
            for n in range(L):
                hid[:, n * F : (n + 1) * F] = activate(x, wg[n], wu[n])
        else:
            span = min(256, L * F)

            def up(n, _):
                cols = pl.ds(pl.multiple_of(n * span, span), span)
                hid[:, cols] = activate(arr[zc].reshape(slots, D), wg[:, cols], wu[:, cols])
                return 0

            if span == L * F:
                hid[...] = activate(x, wg[...], wu[...])
            else:
                lax.fori_loop(0, L * F // span, up, 0)

        def down(n, _):
            cols = pl.ds(pl.multiple_of(n * wide, wide), wide)
            rows_out = jnp.dot(hid[...], wd[:, cols], preferred_element_type=jnp.float32)
            arr[zc, :, :, cols] = rows_out.astype(jnp.bfloat16).reshape(S, two_cap, wide)
            return 0

        lax.fori_loop(0, D // wide, down, 0)

        @pl.when(j > 0)
        def _():
            for ds in range(1, S):
                give_back(zc, ds).start()

    def stage(j, _):
        @pl.when(j < Z)
        def _():
            gather_step(j)

        @pl.when(j >= LAG)
        def _():
            expert_step(j - LAG)

        return 0

    lax.fori_loop(0, Z + LAG, stage, 0)
    for ds in range(1, S):
        give_back(z, ds).start()

    def combine(i, _):
        zc = chip_at(lax.rem(i + 1, Z))
        across(zc).wait_send()

        @pl.when((zc <= z) & (z < Z - 1))
        def _():
            along(zc, 0).wait_send()

        @pl.when((zc >= z) & (z > 0))
        def _():
            along(zc, 1).wait_send()

        for ds in range(1, S):
            give_back(zc, ds).wait_recv()
        back[zc, sp] = arr[zc, sp]
        slot_id = lax.broadcasted_iota(jnp.int32, (2 * rows, slots), 1)
        table = jnp.zeros((2 * rows, slots), jnp.float32)
        for k in range(comb_ref.shape[2]):
            table = jnp.where(
                slot_id == comb_ref[zc, :, k : k + 1], wt_ref[zc, :, k : k + 1], table
            )
        high, low = split_f32(table)

        def mix(n, _):
            cols = pl.ds(pl.multiple_of(n * wide, wide), wide)
            values = back[zc, :, :, cols].reshape(slots, wide)
            total = jnp.dot(high, values, preferred_element_type=jnp.float32)
            total = total + jnp.dot(low, values, preferred_element_type=jnp.float32)
            pbuf[:, :, cols] = total.reshape(2, rows, wide)
            return 0

        lax.fori_loop(0, D // wide, mix, 0)
        gath[2 * zc + 1 - g] = pbuf[1 - g].astype(jnp.bfloat16)
        merge(zc).start()
        merge(zc).wait_recv()

        @pl.when(zc != z)
        def _():
            gath[2 * zc + g] = (pbuf[g] + prem[zc].astype(jnp.float32)).astype(jnp.bfloat16)
            deliver(zc).start()

        return 0

    lax.fori_loop(0, Z, combine, 0)

    def arrived(zc):
        return pltpu.make_async_copy(zrec.at[zc], zrec.at[zc], zs_recv.at[zc])

    for d in range(1, Z):
        arrived(lax.rem(z + d, Z)).wait()

    def finish(n, _):
        at = pl.ds(pl.multiple_of(n * part, part), part)
        total = pbuf[g, at, :] + prem[z, at, :].astype(jnp.float32)
        for d in range(1, Z):
            total = total + zrec[lax.rem(z + d, Z), at, :].astype(jnp.float32)
        mixture = total.astype(jnp.bfloat16)
        out_ref[at, :] = (
            stream[at, :].astype(jnp.float32) + norm_rows(mixture, gain_ref[2:3, :])
        ).astype(jnp.bfloat16)
        return 0

    lax.fori_loop(0, rows // part, finish, 0)
    for i in range(3):
        for d in range(1, L):
            weight_copy(i, d).wait_send()
    for j in range(max(0, Z - ring), Z):
        for ds in range(1, S):
            dispatch(j, ds).wait_send()
    for zc in range(Z):
        for ds in range(1, S):
            give_back(zc, ds).wait_send()
        merge(zc).wait_send()
    for d in range(1, Z):
        deliver(lax.rem(z + d, Z)).wait_send()


def on_device(
    mix_in, gate_in, conv_w, conv_b, decay_param, recur_gate, recur_bias, input_gate, input_bias,
    residual, out_proj, norm_gain, routes, route_wt, exp_gate, exp_up, exp_down,
):
    S, T = lax.axis_size("sp"), lax.axis_size("tp")
    L, D, F = exp_gate.shape
    Z = T // 2
    dims = (S, T, L, Z)
    seq, C = mix_in.shape
    rows = residual.shape[0]
    cap = 2 * rows * routes.shape[1] // (L * S)
    local = lax.rem(lax.axis_index("tp"), L)
    sel, comb, weights = slot_tables(routes, route_wt, dims, rows, cap, local)
    soft = jax.nn.softplus(-decay_param)
    vmem = pl.BlockSpec(memory_space=pltpu.VMEM)
    hbm = pl.BlockSpec(memory_space=pltpu.MemorySpace.HBM)
    b16, f32 = jnp.bfloat16, jnp.float32
    dma = pltpu.SemaphoreType.DMA
    up_shape = (D, L * F) if F % 128 == 0 or L == 1 else (L, D, F)
    return pl.pallas_call(
        functools.partial(layer_kernel, dims),
        out_shape=jax.ShapeDtypeStruct((rows, D), b16),
        in_specs=[vmem] * 14 + [hbm] * 4,
        out_specs=vmem,
        scratch_shapes=[
            pltpu.VMEM((seq + 2 * SUB, C), f32),
            pltpu.VMEM((C, 4 * C), b16),
            pltpu.VMEM((C, 4 * C), b16),
            pltpu.VMEM((seq, C), f32), pltpu.VMEM((seq, C), f32),
            pltpu.VMEM((seq, C), f32), pltpu.VMEM((seq, C), f32),
            pltpu.VMEM((seq, C), b16),
            pltpu.VMEM((rows, T * C), b16),
            pltpu.VMEM(out_proj.shape, b16),
            pltpu.VMEM((rows, D), b16),
            pltpu.VMEM((2, HALO, C), b16),
            pltpu.VMEM((SUB, C), f32),
            pltpu.VMEM((S - 1, SUB, C), f32),
            pltpu.VMEM(up_shape, b16), pltpu.VMEM(up_shape, b16), pltpu.VMEM((L * F, D), b16),
            pltpu.VMEM((S * 2 * cap, L * F), b16),
            pltpu.VMEM((rows, D), b16),
            pltpu.VMEM((T, rows, D), b16),
            pltpu.VMEM((min(Z, RING), S, 2 * cap, D), b16),
            pltpu.VMEM((Z, S, 2 * cap, D), b16),
            pltpu.VMEM((Z, S, 2 * cap, D), b16),
            pltpu.VMEM((Z, rows, D), b16),
            pltpu.VMEM((Z, rows, D), b16),
            pltpu.VMEM((2, rows, D), f32),
            dma, dma((8,)),
            dma((2,)), dma((2,)),
            dma((S - 1,)), dma((S - 1,)),
            dma((T,)), dma((T,)),
            dma((max(L - 1, 1), 3)), dma((max(L - 1, 1), 3)),
            dma((2, Z)), dma((Z,)),
            dma((Z,)), dma((Z,)),
            dma((Z, S - 1)), dma((Z, S - 1)),
            dma((Z, S - 1)), dma((Z, S - 1)),
            dma((Z,)), dma((Z,)),
            dma((Z,)), dma((Z,)),
        ],
        compiler_params=pltpu.CompilerParams(
            collective_id=0, has_side_effects=True, vmem_limit_bytes=62 * 1024 * 1024
        ),
    )(
        mix_in, gate_in, conv_w, conv_b.reshape(1, C), soft, recur_gate, recur_bias, input_gate,
        input_bias, residual, norm_gain, sel, comb, weights, out_proj, exp_gate, exp_up, exp_down,
    )


def solution(mesh):
    return jax.shard_map(
        on_device,
        mesh=mesh,
        in_specs=(
            P("sp", "tp"),
            P("sp", "tp"),
            P(None, "tp"),
            P("tp"),
            P(None, "tp"),
            P(None, "tp", None, None),
            P(None, "tp"),
            P(None, "tp", None, None),
            P(None, "tp"),
            P(("sp", "tp"), None),
            P(),
            P(),
            P("sp", None),
            P("sp", None),
            P("sp", None, "tp"),
            P("sp", None, "tp"),
            P("sp", "tp", None),
        ),
        out_specs=P(("sp", "tp"), None),
        check_vma=False,
    )
```

```python
import functools

import jax
import jax.numpy as jnp
from jax import lax
from jax.experimental import pallas as pl
from jax.experimental.pallas import tpu as pltpu
from jax.sharding import PartitionSpec as P

EPSILON = 1e-06
HIGHEST_MODE = lax.Precision.HIGHEST
MESH = pl.DeviceIdType.MESH
HALO = 16
SUB = 8
RING = 2


def norm_rows(values, gain):
    floats = values.astype(jnp.float32)
    return floats * lax.rsqrt(jnp.mean(floats * floats, axis=-1, keepdims=True) + EPSILON) * gain


def one_minus_exp(y):
    series = -y * (1.0 + y * (1.0 / 2) * (1.0 + y * (1.0 / 3) * (1.0 + y * 0.25 * (1.0 + y * 0.2))))
    return jnp.where(y > -0.1, series, 1.0 - jnp.exp(y))


def split_f32(x):
    high = x.astype(jnp.bfloat16)
    return high, (x - high.astype(jnp.float32)).astype(jnp.bfloat16)


def tile_scan(a, b, reverse):
    row = lax.broadcasted_iota(jnp.int32, a.shape, 1)
    step = 1
    while step < SUB:
        shift = SUB - step if reverse else step
        keep = row < SUB - step if reverse else row >= step
        a_prev = jnp.where(keep, pltpu.roll(a, shift, 1), 1.0)
        b_prev = jnp.where(keep, pltpu.roll(b, shift, 1), 0.0)
        b = b + a * b_prev
        a = a * a_prev
        step *= 2
    return a, b


def layer_kernel(
    dims,
    mix_ref, gate_ref, cw_ref, cb_ref, decay_ref, rg_ref, rb_ref, ig_ref, ib_ref,
    res_ref, gain_ref, routes_ref, wt_ref, op_hbm, eg_hbm, eu_hbm, ed_hbm,
    stream, delta_ref,
    xp, wh, wl, af, bf, ab, bb, mixed, tok, op, proj, halo, summ, ends,
    soft_ref, wg, wu, wd, hid, gath, outg, arr, back, prem, zrec, pin, pbuf,
    op_sem, own_sem, halo_send, halo_recv, sum_send, sum_recv,
    mix_send, mix_recv, w_send, w_recv, p_send, p_recv, ga_send, ga_recv, d2_send, d2_recv,
    dis_send, dis_recv, ret_send, ret_recv, pd_send, pd_recv, zs_send, zs_recv,
    pin_send, pin_recv,
):
    S, T, L, Z = dims
    seq, C = mix_ref.shape
    rows, D = res_ref.shape
    two_cap = arr.shape[2]
    slots = S * two_cap
    heads, hd = rg_ref.shape[1], rg_ref.shape[2]
    F = eg_hbm.shape[2]
    sp = lax.axis_index("sp")
    tp = lax.axis_index("tp")
    z = lax.div(tp, 2)
    g = lax.rem(tp, 2)
    local = 2 * (1 - lax.rem(z, 2)) + g if L > 1 else 0
    upward = z < Z // 2
    inward = jnp.where(upward, z + 1, z - 1)
    middle = (z > 0) & (z < Z - 1) & (L > 1)
    cap = two_cap // 2
    top = routes_ref.shape[0]
    pair_width = 2 * F if L > 1 else F
    partner = tp + 1 - 2 * g

    op_copy = pltpu.make_async_copy(op_hbm, op, op_sem)
    op_copy.start()

    barrier = pltpu.get_barrier_semaphore()
    greeted = 0
    for ds in range(S):
        for dt in range(T):
            if (ds == 0) != (dt == 0):
                pl.semaphore_signal(
                    barrier, inc=1,
                    device_id=(lax.rem(sp + ds, S), lax.rem(tp + dt, T)),
                    device_id_type=MESH,
                )
                greeted += 1

    def remote(src, dst, send, recv, sp_to, tp_to):
        return pltpu.make_async_remote_copy(
            src_ref=src, dst_ref=dst, send_sem=send, recv_sem=recv,
            device_id=(sp_to, tp_to), device_id_type=MESH,
        )

    to_next = remote(mix_ref.at[pl.ds(seq - HALO, HALO)], halo.at[0], halo_send.at[0],
                     halo_recv.at[0], lax.rem(sp + 1, S), tp)
    to_prev = remote(mix_ref.at[pl.ds(0, HALO)], halo.at[1], halo_send.at[1],
                     halo_recv.at[1], lax.rem(sp + S - 1, S), tp)

    tensors = ((eg_hbm, wg, 1), (eu_hbm, wu, 1), (ed_hbm, wd, 0))
    depth = eg_hbm.shape[1]
    pieces = (
        (eg_hbm, wg, 1, 0, depth), (eu_hbm, wu, 1, 0, depth // 2),
        (eu_hbm, wu, 1, depth // 2, depth // 2), (ed_hbm, wd, 0, 0, F),
    )

    def chunk(ref, axis, place):
        if ref.shape[axis] == F:
            return ref
        start = pl.multiple_of(place * F, F)
        return ref.at[:, pl.ds(start, F)] if axis else ref.at[pl.ds(start, F), :]

    def weight_copy(i, core):
        src, dst, axis, first, count = pieces[i]
        side = jnp.where(upward, 0, 1)
        at = pl.ds(first, count)
        return remote(src.at[2 * lax.rem(z, 2) + core].at[at],
                      chunk(dst, axis, 2 + 2 * side + g).at[at],
                      w_send.at[i, core], w_recv.at[i, 2 * side + g], sp, 2 * inward + core)

    def partner_copy(i):
        src, dst, axis = tensors[i]
        return remote(src.at[local + 1 - 2 * g], chunk(dst, axis, g), p_send.at[i],
                      p_recv.at[i], sp, partner)

    own_weights = [
        pltpu.make_async_copy(src.at[local], chunk(dst, axis, g if L > 1 else 0), own_sem.at[i])
        for i, (src, dst, axis) in enumerate(tensors)
    ]

    def start_weights(core, which):
        if L > 1:
            for i in which:
                weight_copy(i, core).start()

    def chip_weights_arrived():
        for i in range(3):
            own_weights[i].wait()
            if L > 1:
                partner_copy(i).wait_recv()

    def weights_arrived(which):
        for i in which:
            for k in range(4):
                _, dst, axis, first, count = pieces[i]
                block = chunk(dst, axis, 2 + k).at[pl.ds(first, count)]
                pltpu.make_async_copy(block, block, w_recv.at[i, k]).wait()

    for c in own_weights:
        c.start()

    wh[...] = jnp.zeros_like(wh)
    wl[...] = jnp.zeros_like(wl)
    for k, ref in enumerate((rg_ref, ig_ref)):
        for sense in range(2):
            for h in range(heads):
                high, low = split_f32(ref[sense, h])
                col = (2 * sense + k) * C + h * hd
                wh[h * hd : (h + 1) * hd, col : col + hd] = high
                wl[h * hd : (h + 1) * hd, col : col + hd] = low
    xp[SUB : SUB + seq, :] = mix_ref[...].astype(jnp.float32)
    soft_ref[...] = jax.nn.softplus(-decay_ref[...])
    pl.semaphore_wait(barrier, greeted)
    to_next.start()
    to_prev.start()
    start_weights(0, (0, 1))
    if L > 1:
        for i in range(3):
            partner_copy(i).start()

    R = min(128, seq)

    def gates(n, _):
        base = pl.multiple_of(n * R, R)
        window = xp[pl.ds(base, R + 2 * SUB), :]
        conv = cb_ref[...] + window[SUB - 2 : SUB - 2 + R] * cw_ref[0:1]
        for tap in range(1, cw_ref.shape[0]):
            conv = conv + window[SUB - 2 + tap : SUB - 2 + tap + R] * cw_ref[tap : tap + 1]
        high, low = split_f32(conv)
        for sense, (a_ref, b_ref) in enumerate(((af, bf), (ab, bb))):
            cols = slice(2 * sense * C, (2 * sense + 2) * C)
            pre = jnp.dot(high, wh[:, cols], preferred_element_type=jnp.float32)
            pre = pre + jnp.dot(low, wh[:, cols], preferred_element_type=jnp.float32)
            pre = pre + jnp.dot(high, wl[:, cols], preferred_element_type=jnp.float32)
            recur = jax.nn.sigmoid(pre[:, :C] + rb_ref[sense : sense + 1])
            inp = jax.nn.sigmoid(pre[:, C:] + ib_ref[sense : sense + 1])
            log_a = -8.0 * recur * soft_ref[sense : sense + 1]
            a = jnp.exp(log_a)
            b = jnp.sqrt(one_minus_exp(2.0 * log_a)) * (inp * conv)
            a, b = tile_scan(
                a.reshape(R // SUB, SUB, C), b.reshape(R // SUB, SUB, C), sense == 1
            )
            a_ref[pl.ds(base, R), :] = a.reshape(R, C)
            b_ref[pl.ds(base, R), :] = b.reshape(R, C)
        return 0

    lax.fori_loop(1, seq // R - 1, gates, 0)
    to_next.wait()
    to_prev.wait()
    tail = halo[0].astype(jnp.float32)[HALO - SUB : HALO]
    head = halo[1].astype(jnp.float32)[0:SUB]
    xp[0:SUB, :] = jnp.where(sp > 0, tail, 0.0)
    xp[SUB + seq : 2 * SUB + seq, :] = jnp.where(sp < S - 1, head, 0.0)
    lax.fori_loop(0, 2, lambda n, _: gates(n * (seq // R - 1), 0), 0)

    tiles = seq // SUB

    def carry(t, held):
        sf, pf, sb, pb = held
        at = pl.ds(pl.multiple_of(t * SUB, SUB), SUB)
        a = af[at, :]
        s = bf[at, :] + a * sf
        p = a * pf
        af[at, :] = p
        bf[at, :] = s
        back = pl.ds(pl.multiple_of((tiles - 1 - t) * SUB, SUB), SUB)
        a = ab[back, :]
        s2 = bb[back, :] + a * sb
        p2 = a * pb
        ab[back, :] = p2
        bb[back, :] = s2
        return s[SUB - 1 : SUB], p[SUB - 1 : SUB], s2[0:1], p2[0:1]

    zero, one = jnp.zeros((1, C), jnp.float32), jnp.ones((1, C), jnp.float32)
    sf, pf, sb, pb = lax.fori_loop(0, tiles, carry, (zero, one, zero, one), unroll=4)
    summ[0:1, :] = sf
    summ[1:2, :] = pf
    summ[2:3, :] = sb
    summ[3:4, :] = pb
    sums = [
        remote(summ, ends.at[ds - 1], sum_send.at[ds - 1], sum_recv.at[ds - 1],
               lax.rem(sp + ds, S), tp)
        for ds in range(1, S)
    ]
    for c in sums:
        c.start()
    for c in sums:
        c.wait()
    fe, be = zero, zero
    for ds in range(S - 1, 0, -1):
        fe = jnp.where(sp >= ds, ends[ds - 1, 1:2, :] * fe + ends[ds - 1, 0:1, :], fe)
    for ds in range(1, S):
        be = jnp.where(sp + S - ds < S, ends[ds - 1, 3:4, :] * be + ends[ds - 1, 2:3, :], be)

    def join(n, _):
        at = pl.ds(pl.multiple_of(n * R, R), R)
        state = (bf[at, :] + af[at, :] * fe) + (bb[at, :] + ab[at, :] * be)
        mixed[at, :] = (state * jax.nn.gelu(gate_ref[at, :].astype(jnp.float32))).astype(
            jnp.bfloat16
        )
        return 0

    lax.fori_loop(0, seq // R, join, 0)

    def block_rows(place):
        return mixed.at[pl.ds(pl.multiple_of(place * rows, rows), rows), :]

    columns = pl.ds(pl.multiple_of(tp * C, C), C)
    moves = []
    for dt in range(1, T):
        to = lax.rem(tp + dt, T)
        moves.append(remote(block_rows(to), tok.at[:, columns], mix_send.at[dt],
                            mix_recv.at[dt], sp, to))
    for c in moves:
        c.start()
    own_move = pltpu.make_async_copy(block_rows(tp), tok.at[:, columns], own_sem.at[6])
    own_move.start()
    start_weights(0, (2,))
    op_copy.wait()
    own_move.wait()
    for c in moves:
        c.wait()

    def project(n, _):
        cols = pl.ds(pl.multiple_of(n * 256, 256), 256)
        proj[:, cols] = (
            jnp.dot(tok[...], op[:, cols], preferred_element_type=jnp.float32)
            .astype(jnp.bfloat16)
        )
        return 0

    lax.fori_loop(0, D // 256, project, 0)
    part = 32

    def norms(n, _):
        at = pl.ds(pl.multiple_of(n * part, part), part)
        s = (
            res_ref[at, :].astype(jnp.float32) + norm_rows(proj[at, :], gain_ref[0:1, :])
        ).astype(jnp.bfloat16)
        stream[at, :] = s
        gath[tp, at, :] = norm_rows(s, gain_ref[1:2, :]).astype(jnp.bfloat16)
        return 0

    lax.fori_loop(0, rows // part, norms, 0)
    wide = min(256, D)

    def chip_at(j):
        low = jnp.minimum(z, Z - 1 - z)
        d = lax.div(j + 1, 2)
        near = jnp.where(lax.rem(j, 2) == 1, z - d, z + d)
        far = jnp.where(z < Z - 1 - z, j, Z - 1 - j)
        return jnp.where(j <= 2 * low, near, far)

    def along(zc, way):
        block = gath.at[2 * zc + g]
        return remote(block, block, ga_send.at[way, zc], ga_recv.at[zc], sp, tp + 2 - 4 * way)

    def across(zc):
        block = gath.at[2 * zc + g]
        return remote(block, block, d2_send.at[zc], d2_recv.at[zc], sp, partner)

    ring = outg.shape[0]

    def dispatch(j, ds):
        zc = chip_at(j)
        to = lax.rem(sp + ds, S)
        return remote(outg.at[lax.rem(j, ring), to], arr.at[zc, sp], dis_send.at[zc, ds - 1],
                      dis_recv.at[zc, ds - 1], to, tp)

    def give_back(zc, ds):
        to = lax.rem(sp + ds, S)
        return remote(arr.at[zc, to], back.at[zc, sp], ret_send.at[zc, ds - 1],
                      ret_recv.at[zc, ds - 1], to, tp)

    def merge(zc):
        return remote(gath.at[2 * zc + 1 - g], prem.at[zc], pd_send.at[zc], pd_recv.at[zc],
                      sp, partner)

    def deliver(zc):
        return remote(gath.at[2 * zc + g], zrec.at[z], zs_send.at[zc], zs_recv.at[z],
                      sp, 2 * zc + g)

    def slot_table(zc, weighted):
        at = pl.ds(pl.multiple_of(zc * (2 * rows), 2 * rows), 2 * rows)
        named, given = routes_ref[:, at], wt_ref[:, at]
        high_rows = max(16, S)
        experts = lax.broadcasted_iota(jnp.int32, (high_rows, 2 * rows), 0) * L + local
        hit = experts == named[0:1]
        share = jnp.where(hit, given[0:1], 0.0)
        for k in range(1, top):
            same = experts == named[k : k + 1]
            hit = hit | same
            share = jnp.where(same, given[k : k + 1], share)
        earlier = lax.broadcasted_iota(jnp.int32, (2 * rows, 2 * rows), 0)
        token = lax.broadcasted_iota(jnp.int32, (2 * rows, 2 * rows), 1)
        inside = jnp.where(token >= rows, rows, 0)
        before = jnp.where((earlier < token) & (earlier >= inside), 1.0, 0.0)
        rank = jnp.dot(
            jnp.where(hit, 1.0, 0.0).astype(jnp.bfloat16), before.astype(jnp.bfloat16),
            preferred_element_type=jnp.float32,
        ).astype(jnp.int32)
        column = lax.broadcasted_iota(jnp.int32, (high_rows, 2 * rows), 1)
        place = jnp.where(hit, rank + jnp.where(column >= rows, cap, 0), -1)
        slot_id = lax.broadcasted_iota(jnp.int32, (two_cap, 2 * rows), 0)
        pieces = [
            jnp.where(slot_id == place[s : s + 1], share[s : s + 1] if weighted else 1.0, 0.0)
            for s in range(S)
        ]
        return jnp.concatenate(pieces, axis=0)

    def gather_step(j):
        zc = chip_at(j)

        @pl.when(j > 0)
        def _():
            pltpu.make_async_copy(gath.at[2 * zc + g], gath.at[2 * zc + g], ga_recv.at[zc]).wait()

        across(zc).start()

        @pl.when((zc <= z) & (z < Z - 1))
        def _():
            along(zc, 0).start()

        @pl.when((zc >= z) & (z > 0))
        def _():
            along(zc, 1).start()

        @pl.when(zc == jnp.where(upward, 0, Z - 1))
        def _():
            start_weights(0, (3,))
            start_weights(1, (0, 1, 2, 3))

        across(zc).wait_recv()
        selector = slot_table(zc, False).astype(jnp.bfloat16)
        slot = lax.rem(j, ring)

        @pl.when(j >= ring)
        def _():
            for ds in range(1, S):
                dispatch(j - ring, ds).wait_send()

        def pick(n, _):
            cols = pl.ds(pl.multiple_of(n * wide, wide), wide)
            tokens = gath[pl.ds(2 * zc, 2), :, cols].reshape(2 * rows, wide)
            picked = jnp.dot(selector, tokens, preferred_element_type=jnp.float32)
            outg[slot, :, :, cols] = picked.astype(jnp.bfloat16).reshape(S, two_cap, wide)
            return 0

        lax.fori_loop(0, D // wide, pick, 0)
        for ds in range(1, S):
            dispatch(j, ds).start()
        arr[zc, sp] = outg[slot, sp]

    def activate(x, gate_w, up_w):
        gate_act = jnp.dot(x, gate_w, preferred_element_type=jnp.float32)
        up_act = jnp.dot(x, up_w, preferred_element_type=jnp.float32)
        return (jax.nn.silu(gate_act) * up_act).astype(jnp.bfloat16)

    def up_part(j, n):
        zc = chip_at(j)
        cols = pl.ds(pl.multiple_of(n * pair_width, pair_width), pair_width)
        if L == 1:
            cols = slice(None)
        hid[j, :, cols] = activate(arr[zc].reshape(slots, D), wg[:, cols], wu[:, cols])

    def down_part(j, depth):
        zc = chip_at(j)

        def down(n, _):
            cols = pl.ds(pl.multiple_of(n * wide, wide), wide)
            rows_out = jnp.dot(
                hid[j, :, :depth], wd[:depth, cols], preferred_element_type=jnp.float32
            )
            arr[zc, :, :, cols] = rows_out.astype(jnp.bfloat16).reshape(S, two_cap, wide)
            return 0

        lax.fori_loop(0, D // wide, down, 0)

    def return_rows(zc):
        for ds in range(1, S):
            give_back(zc, ds).start()

    early = middle & (g == 0)

    def stage(j, _):
        @pl.when(j < Z)
        def _():
            gather_step(j)

        @pl.when(j == 1)
        def _():
            chip_weights_arrived()
            if L > 1:

                @pl.when(early)
                def _():
                    weights_arrived((0, 1, 2))

        @pl.when(j > 0)
        def _():
            for ds in range(1, S):
                dispatch(j - 1, ds).wait_recv()

            def part_of(n, _):
                up_part(j - 1, n)
                return 0

            lax.fori_loop(0, jnp.where(early, 3, 1), part_of, 0)

            @pl.when(jnp.logical_not(middle))
            def _():
                down_part(j - 1, pair_width)

                @pl.when(j > 1)
                def _():
                    return_rows(chip_at(j - 1))

        return 0

    lax.fori_loop(0, Z + 1, stage, 0)

    @pl.when(jnp.logical_not(middle))
    def _():
        return_rows(z)

    if L > 1:

        @pl.when(middle)
        def _():
            @pl.when(g == 1)
            def _():
                weights_arrived((0, 1, 2))

                def rest(n, _):
                    up_part(lax.div(n, 2), 1 + lax.rem(n, 2))
                    return 0

                lax.fori_loop(0, 2 * Z, rest, 0)

            weights_arrived((3,))

            def finish_rows(i, _):
                down_part(Z - 1 - i, 3 * pair_width)
                return_rows(chip_at(Z - 1 - i))
                return 0

            lax.fori_loop(0, Z, finish_rows, 0)

    pair_chip = z + 1 - 2 * lax.rem(z, 2)

    def return_order(i):
        return chip_at(jnp.where(middle, Z - 1 - i, lax.rem(i + 1, Z)))

    def feeds(zc):
        return (zc != z) & (zc != pair_chip) & ((zc > z) == (lax.rem(z, 2) == 0))

    def relays(zc):
        return (zc != z) & (zc != pair_chip) & ((zc > z) != (lax.rem(z, 2) == 0))

    def feed(zc):
        return remote(gath.at[2 * zc + g], pin.at[zc], pin_send.at[zc], pin_recv.at[zc],
                      sp, 2 * pair_chip + g)

    def combine(i, _):
        zc = return_order(i)
        across(zc).wait_send()

        @pl.when((zc <= z) & (z < Z - 1))
        def _():
            along(zc, 0).wait_send()

        @pl.when((zc >= z) & (z > 0))
        def _():
            along(zc, 1).wait_send()

        for ds in range(1, S):
            give_back(zc, ds).wait_recv()
        back[zc, sp] = arr[zc, sp]
        table = jnp.transpose(slot_table(zc, True))
        high, low = split_f32(table)

        def mix(n, _):
            cols = pl.ds(pl.multiple_of(n * wide, wide), wide)
            values = back[zc, :, :, cols].reshape(slots, wide)
            total = jnp.dot(high, values, preferred_element_type=jnp.float32)
            total = total + jnp.dot(low, values, preferred_element_type=jnp.float32)
            pbuf[:, :, cols] = total.reshape(2, rows, wide)
            return 0

        lax.fori_loop(0, D // wide, mix, 0)
        gath[2 * zc + 1 - g] = pbuf[1 - g].astype(jnp.bfloat16)
        merge(zc).start()
        merge(zc).wait_recv()

        @pl.when(feeds(zc) | (zc == pair_chip))
        def _():
            gath[2 * zc + g] = (pbuf[g] + prem[zc].astype(jnp.float32)).astype(jnp.bfloat16)

        @pl.when(feeds(zc))
        def _():
            feed(zc).start()

        @pl.when(relays(zc))
        def _():
            pltpu.make_async_copy(pin.at[zc], pin.at[zc], pin_recv.at[zc]).wait()
            gath[2 * zc + g] = (
                pbuf[g] + prem[zc].astype(jnp.float32) + pin[zc].astype(jnp.float32)
            ).astype(jnp.bfloat16)
            deliver(zc).start()

        @pl.when(zc == pair_chip)
        def _():
            deliver(zc).start()

        return 0

    lax.fori_loop(0, Z, combine, 0)

    def arrived(zc):
        return pltpu.make_async_copy(zrec.at[zc], zrec.at[zc], zs_recv.at[zc])

    senders = [pair_chip]
    for m in range(1, Z // 2):
        other = lax.rem(lax.div(z, 2) + m, Z // 2)
        senders.append(2 * other + jnp.where(2 * other < z, 1, 0))
    for zc in senders:
        arrived(zc).wait()

    def finish(n, _):
        at = pl.ds(pl.multiple_of(n * part, part), part)
        total = pbuf[g, at, :] + prem[z, at, :].astype(jnp.float32)
        for zc in senders:
            total = total + zrec[zc, at, :].astype(jnp.float32)
        mixture = total.astype(jnp.bfloat16)
        delta_ref[at, :] = norm_rows(mixture, gain_ref[2:3, :])
        return 0

    lax.fori_loop(0, rows // part, finish, 0)
    if L > 1:
        for i in range(3):
            partner_copy(i).wait_send()
        for i in range(4):
            for core in range(2):
                weight_copy(i, core).wait_send()
    for j in range(max(0, Z - ring), Z):
        for ds in range(1, S):
            dispatch(j, ds).wait_send()
    for zc in range(Z):
        for ds in range(1, S):
            give_back(zc, ds).wait_send()
        merge(zc).wait_send()

    def drain(i, _):
        zc = return_order(i)

        @pl.when(feeds(zc))
        def _():
            feed(zc).wait_send()

        @pl.when((zc != z) & jnp.logical_not(feeds(zc)))
        def _():
            deliver(zc).wait_send()

        return 0

    lax.fori_loop(0, Z, drain, 0)


def on_device(
    mix_in, gate_in, conv_w, conv_b, decay_param, recur_gate, recur_bias, input_gate, input_bias,
    residual, out_proj, norm_gain, routes, route_wt, exp_gate, exp_up, exp_down,
):
    S, T = lax.axis_size("sp"), lax.axis_size("tp")
    L, D, F = exp_gate.shape
    Z = T // 2
    dims = (S, T, L, Z)
    seq, C = mix_in.shape
    rows = residual.shape[0]
    cap = 2 * rows * routes.shape[1] // (L * S)
    vmem = pl.BlockSpec(memory_space=pltpu.VMEM)
    hbm = pl.BlockSpec(memory_space=pltpu.MemorySpace.HBM)
    b16, f32 = jnp.bfloat16, jnp.float32
    dma = pltpu.SemaphoreType.DMA
    hidden = 6 * F if L > 1 else F
    up_shape = (D, hidden)
    stream, delta = pl.pallas_call(
        functools.partial(layer_kernel, dims),
        out_shape=(jax.ShapeDtypeStruct((rows, D), b16), jax.ShapeDtypeStruct((rows, D), f32)),
        in_specs=[vmem] * 13 + [hbm] * 4,
        out_specs=(vmem, vmem),
        scratch_shapes=[
            pltpu.VMEM((seq + 2 * SUB, C), f32),
            pltpu.VMEM((C, 4 * C), b16),
            pltpu.VMEM((C, 4 * C), b16),
            pltpu.VMEM((seq, C), f32), pltpu.VMEM((seq, C), f32),
            pltpu.VMEM((seq, C), f32), pltpu.VMEM((seq, C), f32),
            pltpu.VMEM((seq, C), b16),
            pltpu.VMEM((rows, T * C), b16),
            pltpu.VMEM(out_proj.shape, b16),
            pltpu.VMEM((rows, D), b16),
            pltpu.VMEM((2, HALO, C), b16),
            pltpu.VMEM((SUB, C), f32),
            pltpu.VMEM((S - 1, SUB, C), f32),
            pltpu.VMEM((2, C), f32),
            pltpu.VMEM(up_shape, b16), pltpu.VMEM(up_shape, b16), pltpu.VMEM((hidden, D), b16),
            pltpu.VMEM((Z, S * 2 * cap, hidden), b16),
            pltpu.VMEM((T, rows, D), b16),
            pltpu.VMEM((min(Z, RING), S, 2 * cap, D), b16),
            pltpu.VMEM((Z, S, 2 * cap, D), b16),
            pltpu.VMEM((Z, S, 2 * cap, D), b16),
            pltpu.VMEM((Z, rows, D), b16),
            pltpu.VMEM((Z, rows, D), b16),
            pltpu.VMEM((Z, rows, D), b16),
            pltpu.VMEM((2, rows, D), f32),
            dma, dma((8,)),
            dma((2,)), dma((2,)),
            dma((S - 1,)), dma((S - 1,)),
            dma((T,)), dma((T,)),
            dma((4, 2)), dma((4, 4)),
            dma((3,)), dma((3,)),
            dma((2, Z)), dma((Z,)),
            dma((Z,)), dma((Z,)),
            dma((Z, S - 1)), dma((Z, S - 1)),
            dma((Z, S - 1)), dma((Z, S - 1)),
            dma((Z,)), dma((Z,)),
            dma((Z,)), dma((Z,)),
            dma((Z,)), dma((Z,)),
        ],
        compiler_params=pltpu.CompilerParams(
            collective_id=0, has_side_effects=True, vmem_limit_bytes=63 * 1024 * 1024
        ),
    )(
        mix_in, gate_in, conv_w, conv_b.reshape(1, C), decay_param, recur_gate, recur_bias,
        input_gate, input_bias, residual, norm_gain, routes.T, route_wt.T, out_proj,
        exp_gate, exp_up, exp_down,
    )
    return (stream.astype(f32) + delta).astype(b16)


def solution(mesh):
    return jax.shard_map(
        on_device,
        mesh=mesh,
        in_specs=(
            P("sp", "tp"),
            P("sp", "tp"),
            P(None, "tp"),
            P("tp"),
            P(None, "tp"),
            P(None, "tp", None, None),
            P(None, "tp"),
            P(None, "tp", None, None),
            P(None, "tp"),
            P(("sp", "tp"), None),
            P(),
            P(),
            P("sp", None),
            P("sp", None),
            P("sp", None, "tp"),
            P("sp", None, "tp"),
            P("sp", "tp", None),
        ),
        out_specs=P(("sp", "tp"), None),
        check_vma=False,
    )
```

```python
import functools

import jax
import jax.numpy as jnp
from jax import lax
from jax.experimental import pallas as pl
from jax.experimental.pallas import tpu as pltpu
from jax.sharding import PartitionSpec as P

EPSILON = 1e-06
HIGHEST_MODE = lax.Precision.HIGHEST
MESH = pl.DeviceIdType.MESH
HALO = 16
SUB = 8
RING = 2


def norm_rows(values, gain):
    floats = values.astype(jnp.float32)
    return floats * lax.rsqrt(jnp.mean(floats * floats, axis=-1, keepdims=True) + EPSILON) * gain


def one_minus_exp(y):
    series = -y * (1.0 + y * (1.0 / 2) * (1.0 + y * (1.0 / 3) * (1.0 + y * 0.25 * (1.0 + y * 0.2))))
    return jnp.where(y > -0.1, series, 1.0 - jnp.exp(y))


def split_f32(x):
    high = x.astype(jnp.bfloat16)
    return high, (x - high.astype(jnp.float32)).astype(jnp.bfloat16)


def tile_scan(a, b, reverse):
    row = lax.broadcasted_iota(jnp.int32, a.shape, 1)
    step = 1
    while step < SUB:
        shift = SUB - step if reverse else step
        keep = row < SUB - step if reverse else row >= step
        a_prev = jnp.where(keep, pltpu.roll(a, shift, 1), 1.0)
        b_prev = jnp.where(keep, pltpu.roll(b, shift, 1), 0.0)
        b = b + a * b_prev
        a = a * a_prev
        step *= 2
    return a, b


def layer_kernel(
    dims,
    mix_ref, gate_ref, cw_ref, cb_ref, decay_ref, rg_ref, rb_ref, ig_ref, ib_ref,
    res_ref, gain_ref, routes_ref, wt_ref, op_hbm, eg_hbm, eu_hbm, ed_hbm,
    stream, delta_ref,
    xp, wh, wl, af, bf, ab, bb, mixed, tok, op, proj, halo, summ, ends,
    soft_ref, wg, wu, wd, hid, gath, outg, arr, back, prem, zrec, pin, pbuf,
    op_sem, own_sem, halo_send, halo_recv, sum_send, sum_recv,
    mix_send, mix_recv, w_send, w_recv, p_send, p_recv, ga_send, ga_recv, d2_send, d2_recv,
    dis_send, dis_recv, ret_send, ret_recv, pd_send, pd_recv, zs_send, zs_recv,
    pin_send, pin_recv,
):
    S, T, L, Z = dims
    seq, C = mix_ref.shape
    rows, D = res_ref.shape
    two_cap = arr.shape[2]
    slots = S * two_cap
    heads, hd = rg_ref.shape[1], rg_ref.shape[2]
    F = eg_hbm.shape[2]
    sp = lax.axis_index("sp")
    tp = lax.axis_index("tp")
    z = lax.div(tp, 2)
    g = lax.rem(tp, 2)
    local = 2 * (1 - lax.rem(z, 2)) + g if L > 1 else 0
    upward = z < Z // 2
    inward = jnp.where(upward, z + 1, z - 1)
    middle = (z > 0) & (z < Z - 1) & (L > 1)
    cap = two_cap // 2
    top = routes_ref.shape[0]
    pair_width = 2 * F if L > 1 else F
    partner = tp + 1 - 2 * g

    op_copy = pltpu.make_async_copy(op_hbm, op, op_sem)
    op_copy.start()

    barrier = pltpu.get_barrier_semaphore()
    greeted = 0
    for ds in range(S):
        for dt in range(T):
            if (ds == 0) != (dt == 0):
                pl.semaphore_signal(
                    barrier, inc=1,
                    device_id=(lax.rem(sp + ds, S), lax.rem(tp + dt, T)),
                    device_id_type=MESH,
                )
                greeted += 1

    def remote(src, dst, send, recv, sp_to, tp_to):
        return pltpu.make_async_remote_copy(
            src_ref=src, dst_ref=dst, send_sem=send, recv_sem=recv,
            device_id=(sp_to, tp_to), device_id_type=MESH,
        )

    to_next = remote(mix_ref.at[pl.ds(seq - HALO, HALO)], halo.at[0], halo_send.at[0],
                     halo_recv.at[0], lax.rem(sp + 1, S), tp)
    to_prev = remote(mix_ref.at[pl.ds(0, HALO)], halo.at[1], halo_send.at[1],
                     halo_recv.at[1], lax.rem(sp + S - 1, S), tp)

    tensors = ((eg_hbm, wg, 1), (eu_hbm, wu, 1), (ed_hbm, wd, 0))
    depth = eg_hbm.shape[1]
    pieces = (
        (eg_hbm, wg, 1, 0, depth), (eu_hbm, wu, 1, 0, depth // 2),
        (eu_hbm, wu, 1, depth // 2, depth // 2), (ed_hbm, wd, 0, 0, F),
    )

    def chunk(ref, axis, place):
        if ref.shape[axis] == F:
            return ref
        start = pl.multiple_of(place * F, F)
        return ref.at[:, pl.ds(start, F)] if axis else ref.at[pl.ds(start, F), :]

    def weight_copy(i, core):
        src, dst, axis, first, count = pieces[i]
        side = jnp.where(upward, 0, 1)
        at = pl.ds(first, count)
        return remote(src.at[2 * lax.rem(z, 2) + core].at[at],
                      chunk(dst, axis, 2 + 2 * side + g).at[at],
                      w_send.at[i, core], w_recv.at[i, 2 * side + g], sp, 2 * inward + core)

    def partner_copy(i):
        src, dst, axis = tensors[i]
        return remote(src.at[local + 1 - 2 * g], chunk(dst, axis, g), p_send.at[i],
                      p_recv.at[i], sp, partner)

    own_weights = [
        pltpu.make_async_copy(src.at[local], chunk(dst, axis, g if L > 1 else 0), own_sem.at[i])
        for i, (src, dst, axis) in enumerate(tensors)
    ]

    def start_weights(core, which):
        if L > 1:
            for i in which:
                weight_copy(i, core).start()

    def chip_weights_arrived():
        for i in range(3):
            own_weights[i].wait()
            if L > 1:
                partner_copy(i).wait_recv()

    def weights_arrived(which):
        for i in which:
            for k in range(4):
                _, dst, axis, first, count = pieces[i]
                block = chunk(dst, axis, 2 + k).at[pl.ds(first, count)]
                pltpu.make_async_copy(block, block, w_recv.at[i, k]).wait()

    for c in own_weights:
        c.start()

    wh[...] = jnp.zeros_like(wh)
    wl[...] = jnp.zeros_like(wl)
    for k, ref in enumerate((rg_ref, ig_ref)):
        for sense in range(2):
            for h in range(heads):
                high, low = split_f32(ref[sense, h])
                col = (2 * sense + k) * C + h * hd
                wh[h * hd : (h + 1) * hd, col : col + hd] = high
                wl[h * hd : (h + 1) * hd, col : col + hd] = low
    xp[SUB : SUB + seq, :] = mix_ref[...].astype(jnp.float32)
    soft_ref[...] = jax.nn.softplus(-decay_ref[...])
    pl.semaphore_wait(barrier, greeted)
    to_next.start()
    to_prev.start()
    start_weights(0, (0, 1))
    if L > 1:
        for i in range(3):
            partner_copy(i).start()

    R = min(128, seq)

    def gates(n, _):
        base = pl.multiple_of(n * R, R)
        window = xp[pl.ds(base, R + 2 * SUB), :]
        conv = cb_ref[...] + window[SUB - 2 : SUB - 2 + R] * cw_ref[0:1]
        for tap in range(1, cw_ref.shape[0]):
            conv = conv + window[SUB - 2 + tap : SUB - 2 + tap + R] * cw_ref[tap : tap + 1]
        high, low = split_f32(conv)
        for sense, (a_ref, b_ref) in enumerate(((af, bf), (ab, bb))):
            cols = slice(2 * sense * C, (2 * sense + 2) * C)
            pre = jnp.dot(high, wh[:, cols], preferred_element_type=jnp.float32)
            pre = pre + jnp.dot(low, wh[:, cols], preferred_element_type=jnp.float32)
            pre = pre + jnp.dot(high, wl[:, cols], preferred_element_type=jnp.float32)
            recur = jax.nn.sigmoid(pre[:, :C] + rb_ref[sense : sense + 1])
            inp = jax.nn.sigmoid(pre[:, C:] + ib_ref[sense : sense + 1])
            log_a = -8.0 * recur * soft_ref[sense : sense + 1]
            a = jnp.exp(log_a)
            b = jnp.sqrt(one_minus_exp(2.0 * log_a)) * (inp * conv)
            a, b = tile_scan(
                a.reshape(R // SUB, SUB, C), b.reshape(R // SUB, SUB, C), sense == 1
            )
            a_ref[pl.ds(base, R), :] = a.reshape(R, C)
            b_ref[pl.ds(base, R), :] = b.reshape(R, C)
        return 0

    lax.fori_loop(1, seq // R - 1, gates, 0)
    to_next.wait()
    to_prev.wait()
    tail = halo[0].astype(jnp.float32)[HALO - SUB : HALO]
    head = halo[1].astype(jnp.float32)[0:SUB]
    xp[0:SUB, :] = jnp.where(sp > 0, tail, 0.0)
    xp[SUB + seq : 2 * SUB + seq, :] = jnp.where(sp < S - 1, head, 0.0)
    lax.fori_loop(0, 2, lambda n, _: gates(n * (seq // R - 1), 0), 0)

    tiles = seq // SUB

    def carry(t, held):
        sf, pf, sb, pb = held
        at = pl.ds(pl.multiple_of(t * SUB, SUB), SUB)
        a = af[at, :]
        s = bf[at, :] + a * sf
        p = a * pf
        af[at, :] = p
        bf[at, :] = s
        back = pl.ds(pl.multiple_of((tiles - 1 - t) * SUB, SUB), SUB)
        a = ab[back, :]
        s2 = bb[back, :] + a * sb
        p2 = a * pb
        ab[back, :] = p2
        bb[back, :] = s2
        return s[SUB - 1 : SUB], p[SUB - 1 : SUB], s2[0:1], p2[0:1]

    zero, one = jnp.zeros((1, C), jnp.float32), jnp.ones((1, C), jnp.float32)
    sf, pf, sb, pb = lax.fori_loop(0, tiles, carry, (zero, one, zero, one), unroll=4)
    summ[0:1, :] = sf
    summ[1:2, :] = pf
    summ[2:3, :] = sb
    summ[3:4, :] = pb
    sums = [
        remote(summ, ends.at[ds - 1], sum_send.at[ds - 1], sum_recv.at[ds - 1],
               lax.rem(sp + ds, S), tp)
        for ds in range(1, S)
    ]
    for c in sums:
        c.start()
    for c in sums:
        c.wait()
    fe, be = zero, zero
    for ds in range(S - 1, 0, -1):
        fe = jnp.where(sp >= ds, ends[ds - 1, 1:2, :] * fe + ends[ds - 1, 0:1, :], fe)
    for ds in range(1, S):
        be = jnp.where(sp + S - ds < S, ends[ds - 1, 3:4, :] * be + ends[ds - 1, 2:3, :], be)

    def join(n, _):
        at = pl.ds(pl.multiple_of(n * R, R), R)
        state = (bf[at, :] + af[at, :] * fe) + (bb[at, :] + ab[at, :] * be)
        mixed[at, :] = (state * jax.nn.gelu(gate_ref[at, :].astype(jnp.float32))).astype(
            jnp.bfloat16
        )
        return 0

    lax.fori_loop(0, seq // R, join, 0)

    def block_rows(place):
        return mixed.at[pl.ds(pl.multiple_of(place * rows, rows), rows), :]

    columns = pl.ds(pl.multiple_of(tp * C, C), C)
    moves = []
    for dt in range(1, T):
        to = lax.rem(tp + dt, T)
        moves.append(remote(block_rows(to), tok.at[:, columns], mix_send.at[dt],
                            mix_recv.at[dt], sp, to))
    for c in moves:
        c.start()
    own_move = pltpu.make_async_copy(block_rows(tp), tok.at[:, columns], own_sem.at[6])
    own_move.start()
    start_weights(0, (2,))
    op_copy.wait()
    own_move.wait()
    for c in moves:
        c.wait()

    def project(n, _):
        cols = pl.ds(pl.multiple_of(n * 256, 256), 256)
        proj[:, cols] = (
            jnp.dot(tok[...], op[:, cols], preferred_element_type=jnp.float32)
            .astype(jnp.bfloat16)
        )
        return 0

    lax.fori_loop(0, D // 256, project, 0)
    part = 32

    def norms(n, _):
        at = pl.ds(pl.multiple_of(n * part, part), part)
        s = (
            res_ref[at, :].astype(jnp.float32) + norm_rows(proj[at, :], gain_ref[0:1, :])
        ).astype(jnp.bfloat16)
        stream[at, :] = s
        gath[tp, at, :] = norm_rows(s, gain_ref[1:2, :]).astype(jnp.bfloat16)
        return 0

    lax.fori_loop(0, rows // part, norms, 0)
    wide = min(256, D)

    def chip_at(j):
        low = jnp.minimum(z, Z - 1 - z)
        d = lax.div(j + 1, 2)
        near = jnp.where(lax.rem(j, 2) == 1, z - d, z + d)
        far = jnp.where(z < Z - 1 - z, j, Z - 1 - j)
        return jnp.where(j <= 2 * low, near, far)

    def along(zc, way):
        block = gath.at[2 * zc + g]
        return remote(block, block, ga_send.at[way, zc], ga_recv.at[zc], sp, tp + 2 - 4 * way)

    def across(zc):
        block = gath.at[2 * zc + g]
        return remote(block, block, d2_send.at[zc], d2_recv.at[zc], sp, partner)

    ring = outg.shape[0]

    def dispatch(j, ds):
        zc = chip_at(j)
        to = lax.rem(sp + ds, S)
        return remote(outg.at[lax.rem(j, ring), to], arr.at[zc, sp], dis_send.at[zc, ds - 1],
                      dis_recv.at[zc, ds - 1], to, tp)

    def give_back(zc, ds):
        to = lax.rem(sp + ds, S)
        return remote(arr.at[zc, to], back.at[zc, sp], ret_send.at[zc, ds - 1],
                      ret_recv.at[zc, ds - 1], to, tp)

    def merge(zc):
        return remote(gath.at[2 * zc + 1 - g], prem.at[zc], pd_send.at[zc], pd_recv.at[zc],
                      sp, partner)

    def half_at(h):
        return pl.ds(h * (rows // 2), rows // 2)

    def deliver(zc, h):
        at = half_at(h)
        return remote(gath.at[2 * zc + g, at], zrec.at[z, at], zs_send.at[zc, h],
                      zs_recv.at[z, h], sp, 2 * zc + g)

    def slot_table(zc, weighted):
        at = pl.ds(pl.multiple_of(zc * (2 * rows), 2 * rows), 2 * rows)
        named, given = routes_ref[:, at], wt_ref[:, at]
        high_rows = max(16, S)
        experts = lax.broadcasted_iota(jnp.int32, (high_rows, 2 * rows), 0) * L + local
        hit = experts == named[0:1]
        share = jnp.where(hit, given[0:1], 0.0)
        for k in range(1, top):
            same = experts == named[k : k + 1]
            hit = hit | same
            share = jnp.where(same, given[k : k + 1], share)
        earlier = lax.broadcasted_iota(jnp.int32, (2 * rows, 2 * rows), 0)
        token = lax.broadcasted_iota(jnp.int32, (2 * rows, 2 * rows), 1)
        inside = jnp.where(token >= rows, rows, 0)
        before = jnp.where((earlier < token) & (earlier >= inside), 1.0, 0.0)
        rank = jnp.dot(
            jnp.where(hit, 1.0, 0.0).astype(jnp.bfloat16), before.astype(jnp.bfloat16),
            preferred_element_type=jnp.float32,
        ).astype(jnp.int32)
        column = lax.broadcasted_iota(jnp.int32, (high_rows, 2 * rows), 1)
        place = jnp.where(hit, rank + jnp.where(column >= rows, cap, 0), -1)
        slot_id = lax.broadcasted_iota(jnp.int32, (two_cap, 2 * rows), 0)
        pieces = [
            jnp.where(slot_id == place[s : s + 1], share[s : s + 1] if weighted else 1.0, 0.0)
            for s in range(S)
        ]
        return jnp.concatenate(pieces, axis=0)

    def gather_step(j):
        zc = chip_at(j)

        @pl.when(j > 0)
        def _():
            pltpu.make_async_copy(gath.at[2 * zc + g], gath.at[2 * zc + g], ga_recv.at[zc]).wait()

        across(zc).start()

        @pl.when((zc <= z) & (z < Z - 1))
        def _():
            along(zc, 0).start()

        @pl.when((zc >= z) & (z > 0))
        def _():
            along(zc, 1).start()

        @pl.when(zc == jnp.where(upward, 0, Z - 1))
        def _():
            start_weights(0, (3,))
            start_weights(1, (0, 1, 2, 3))

        across(zc).wait_recv()
        selector = slot_table(zc, False).astype(jnp.bfloat16)
        slot = lax.rem(j, ring)

        @pl.when(j >= ring)
        def _():
            for ds in range(1, S):
                dispatch(j - ring, ds).wait_send()

        def pick(n, _):
            cols = pl.ds(pl.multiple_of(n * wide, wide), wide)
            tokens = gath[pl.ds(2 * zc, 2), :, cols].reshape(2 * rows, wide)
            picked = jnp.dot(selector, tokens, preferred_element_type=jnp.float32)
            outg[slot, :, :, cols] = picked.astype(jnp.bfloat16).reshape(S, two_cap, wide)
            return 0

        lax.fori_loop(0, D // wide, pick, 0)
        for ds in range(1, S):
            dispatch(j, ds).start()
        arr[zc, sp] = outg[slot, sp]

    def activate(x, gate_w, up_w):
        gate_act = jnp.dot(x, gate_w, preferred_element_type=jnp.float32)
        up_act = jnp.dot(x, up_w, preferred_element_type=jnp.float32)
        return (jax.nn.silu(gate_act) * up_act).astype(jnp.bfloat16)

    def up_part(j, n):
        zc = chip_at(j)
        cols = pl.ds(pl.multiple_of(n * pair_width, pair_width), pair_width)
        if L == 1:
            cols = slice(None)
        hid[zc, :, cols] = activate(arr[zc].reshape(slots, D), wg[:, cols], wu[:, cols])

    def down_part(zc, depth):
        def down(n, _):
            cols = pl.ds(pl.multiple_of(n * wide, wide), wide)
            rows_out = jnp.dot(
                hid[zc, :, :depth], wd[:depth, cols], preferred_element_type=jnp.float32
            )
            arr[zc, :, :, cols] = rows_out.astype(jnp.bfloat16).reshape(S, two_cap, wide)
            return 0

        lax.fori_loop(0, D // wide, down, 0)

    def return_rows(zc):
        for ds in range(1, S):
            give_back(zc, ds).start()

    early = middle & (g == 0)

    def return_order(i):
        return chip_at(lax.rem(i + 1, Z))

    def stage(j, _):
        @pl.when(j < Z)
        def _():
            gather_step(j)

        @pl.when(j == 1)
        def _():
            chip_weights_arrived()
            if L > 1:

                @pl.when(early)
                def _():
                    weights_arrived((0, 1, 2))

        @pl.when(j > 0)
        def _():
            for ds in range(1, S):
                dispatch(j - 1, ds).wait_recv()

            def part_of(n, _):
                up_part(j - 1, n)
                return 0

            lax.fori_loop(0, jnp.where(early, 3, 1), part_of, 0)

            @pl.when(jnp.logical_not(middle))
            def _():
                down_part(chip_at(j - 1), pair_width)

                @pl.when(j > 1)
                def _():
                    return_rows(chip_at(j - 1))

        return 0

    lax.fori_loop(0, Z + 1, stage, 0)

    @pl.when(jnp.logical_not(middle))
    def _():
        return_rows(z)

    if L > 1:

        @pl.when(middle)
        def _():
            @pl.when(g == 1)
            def _():
                weights_arrived((0, 1, 2))

                def rest(n, _):
                    up_part(lax.div(n, 2), 1 + lax.rem(n, 2))
                    return 0

                lax.fori_loop(0, 2 * Z, rest, 0)

            weights_arrived((3,))

            def finish_rows(i, _):
                down_part(return_order(i), 3 * pair_width)
                return_rows(return_order(i))
                return 0

            lax.fori_loop(0, Z, finish_rows, 0)

    pair_chip = z + 1 - 2 * lax.rem(z, 2)

    def feeds(zc):
        return (zc != z) & (zc != pair_chip) & ((zc > z) == (lax.rem(z, 2) == 0))

    def relays(zc):
        return (zc != z) & (zc != pair_chip) & ((zc > z) != (lax.rem(z, 2) == 0))

    def feed(zc, h):
        at = half_at(h)
        return remote(gath.at[2 * zc + g, at], pin.at[zc, at], pin_send.at[zc, h],
                      pin_recv.at[zc, h], sp, 2 * pair_chip + g)

    def combine(i, _):
        zc = return_order(i)
        across(zc).wait_send()

        @pl.when((zc <= z) & (z < Z - 1))
        def _():
            along(zc, 0).wait_send()

        @pl.when((zc >= z) & (z > 0))
        def _():
            along(zc, 1).wait_send()

        table = jnp.transpose(slot_table(zc, True))
        high, low = split_f32(table)
        for ds in range(1, S):
            give_back(zc, ds).wait_recv()
        back[zc, sp] = arr[zc, sp]

        def mix(n, _):
            cols = pl.ds(pl.multiple_of(n * wide, wide), wide)
            values = back[zc, :, :, cols].reshape(slots, wide)
            total = jnp.dot(high, values, preferred_element_type=jnp.float32)
            total = total + jnp.dot(low, values, preferred_element_type=jnp.float32)
            pbuf[:, :, cols] = total.reshape(2, rows, wide)
            return 0

        lax.fori_loop(0, D // wide, mix, 0)
        gath[2 * zc + 1 - g] = pbuf[1 - g].astype(jnp.bfloat16)
        merge(zc).start()
        merge(zc).wait_recv()

        for h in range(2):
            at = half_at(h)

            @pl.when(relays(zc))
            def _():
                pltpu.make_async_copy(pin.at[zc, at], pin.at[zc, at], pin_recv.at[zc, h]).wait()
                gath[2 * zc + g, at] = (
                    pbuf[g, at] + prem[zc, at].astype(jnp.float32)
                    + pin[zc, at].astype(jnp.float32)
                ).astype(jnp.bfloat16)

            @pl.when(feeds(zc) | (zc == pair_chip))
            def _():
                gath[2 * zc + g, at] = (
                    pbuf[g, at] + prem[zc, at].astype(jnp.float32)
                ).astype(jnp.bfloat16)

            @pl.when(feeds(zc))
            def _():
                feed(zc, h).start()

            @pl.when(relays(zc) | (zc == pair_chip))
            def _():
                deliver(zc, h).start()

        return 0

    lax.fori_loop(0, Z, combine, 0)

    senders = [pair_chip]
    for m in range(1, Z // 2):
        other = lax.rem(lax.div(z, 2) + m, Z // 2)
        senders.append(2 * other + jnp.where(2 * other < z, 1, 0))
    for zc in senders:
        for h in range(2):
            block = zrec.at[zc, half_at(h)]
            pltpu.make_async_copy(block, block, zs_recv.at[zc, h]).wait()

    def finish(n, _):
        at = pl.ds(pl.multiple_of(n * part, part), part)
        total = pbuf[g, at, :] + prem[z, at, :].astype(jnp.float32)
        for zc in senders:
            total = total + zrec[zc, at, :].astype(jnp.float32)
        mixture = total.astype(jnp.bfloat16)
        delta_ref[at, :] = norm_rows(mixture, gain_ref[2:3, :])
        return 0

    lax.fori_loop(0, rows // part, finish, 0)
    if L > 1:
        for i in range(3):
            partner_copy(i).wait_send()
        for i in range(4):
            for core in range(2):
                weight_copy(i, core).wait_send()
    for j in range(max(0, Z - ring), Z):
        for ds in range(1, S):
            dispatch(j, ds).wait_send()
    for zc in range(Z):
        for ds in range(1, S):
            give_back(zc, ds).wait_send()
        merge(zc).wait_send()

    def drain(i, _):
        zc = return_order(i)

        @pl.when(feeds(zc))
        def _():
            for h in range(2):
                feed(zc, h).wait_send()

        @pl.when((zc != z) & jnp.logical_not(feeds(zc)))
        def _():
            for h in range(2):
                deliver(zc, h).wait_send()

        return 0

    lax.fori_loop(0, Z, drain, 0)


def on_device(
    mix_in, gate_in, conv_w, conv_b, decay_param, recur_gate, recur_bias, input_gate, input_bias,
    residual, out_proj, norm_gain, routes, route_wt, exp_gate, exp_up, exp_down,
):
    S, T = lax.axis_size("sp"), lax.axis_size("tp")
    L, D, F = exp_gate.shape
    Z = T // 2
    dims = (S, T, L, Z)
    seq, C = mix_in.shape
    rows = residual.shape[0]
    cap = 2 * rows * routes.shape[1] // (L * S)
    vmem = pl.BlockSpec(memory_space=pltpu.VMEM)
    hbm = pl.BlockSpec(memory_space=pltpu.MemorySpace.HBM)
    b16, f32 = jnp.bfloat16, jnp.float32
    dma = pltpu.SemaphoreType.DMA
    hidden = 6 * F if L > 1 else F
    up_shape = (D, hidden)
    stream, delta = pl.pallas_call(
        functools.partial(layer_kernel, dims),
        out_shape=(jax.ShapeDtypeStruct((rows, D), b16), jax.ShapeDtypeStruct((rows, D), f32)),
        in_specs=[vmem] * 13 + [hbm] * 4,
        out_specs=(vmem, vmem),
        scratch_shapes=[
            pltpu.VMEM((seq + 2 * SUB, C), f32),
            pltpu.VMEM((C, 4 * C), b16),
            pltpu.VMEM((C, 4 * C), b16),
            pltpu.VMEM((seq, C), f32), pltpu.VMEM((seq, C), f32),
            pltpu.VMEM((seq, C), f32), pltpu.VMEM((seq, C), f32),
            pltpu.VMEM((seq, C), b16),
            pltpu.VMEM((rows, T * C), b16),
            pltpu.VMEM(out_proj.shape, b16),
            pltpu.VMEM((rows, D), b16),
            pltpu.VMEM((2, HALO, C), b16),
            pltpu.VMEM((SUB, C), f32),
            pltpu.VMEM((S - 1, SUB, C), f32),
            pltpu.VMEM((2, C), f32),
            pltpu.VMEM(up_shape, b16), pltpu.VMEM(up_shape, b16), pltpu.VMEM((hidden, D), b16),
            pltpu.VMEM((Z, S * 2 * cap, hidden), b16),
            pltpu.VMEM((T, rows, D), b16),
            pltpu.VMEM((min(Z, RING), S, 2 * cap, D), b16),
            pltpu.VMEM((Z, S, 2 * cap, D), b16),
            pltpu.VMEM((Z, S, 2 * cap, D), b16),
            pltpu.VMEM((Z, rows, D), b16),
            pltpu.VMEM((Z, rows, D), b16),
            pltpu.VMEM((Z, rows, D), b16),
            pltpu.VMEM((2, rows, D), f32),
            dma, dma((8,)),
            dma((2,)), dma((2,)),
            dma((S - 1,)), dma((S - 1,)),
            dma((T,)), dma((T,)),
            dma((4, 2)), dma((4, 4)),
            dma((3,)), dma((3,)),
            dma((2, Z)), dma((Z,)),
            dma((Z,)), dma((Z,)),
            dma((Z, S - 1)), dma((Z, S - 1)),
            dma((Z, S - 1)), dma((Z, S - 1)),
            dma((Z,)), dma((Z,)),
            dma((Z, 2)), dma((Z, 2)),
            dma((Z, 2)), dma((Z, 2)),
        ],
        compiler_params=pltpu.CompilerParams(
            collective_id=0, has_side_effects=True, vmem_limit_bytes=63 * 1024 * 1024
        ),
    )(
        mix_in, gate_in, conv_w, conv_b.reshape(1, C), decay_param, recur_gate, recur_bias,
        input_gate, input_bias, residual, norm_gain, routes.T, route_wt.T, out_proj,
        exp_gate, exp_up, exp_down,
    )
    return (stream.astype(f32) + delta).astype(b16)


def solution(mesh):
    return jax.shard_map(
        on_device,
        mesh=mesh,
        in_specs=(
            P("sp", "tp"),
            P("sp", "tp"),
            P(None, "tp"),
            P("tp"),
            P(None, "tp"),
            P(None, "tp", None, None),
            P(None, "tp"),
            P(None, "tp", None, None),
            P(None, "tp"),
            P(("sp", "tp"), None),
            P(),
            P(),
            P("sp", None),
            P("sp", None),
            P("sp", None, "tp"),
            P("sp", None, "tp"),
            P("sp", "tp", None),
        ),
        out_specs=P(("sp", "tp"), None),
        check_vma=False,
    )
```

```python
import functools

import jax
import jax.numpy as jnp
from jax import lax
from jax.experimental import pallas as pl
from jax.experimental.pallas import tpu as pltpu
from jax.sharding import PartitionSpec as P

EPSILON = 1e-06
HIGHEST_MODE = lax.Precision.HIGHEST
MESH = pl.DeviceIdType.MESH
HALO = 16
SUB = 8
RING = 2


def norm_rows(values, gain):
    floats = values.astype(jnp.float32)
    return floats * lax.rsqrt(jnp.mean(floats * floats, axis=-1, keepdims=True) + EPSILON) * gain


def one_minus_exp(y):
    series = -y * (1.0 + y * (1.0 / 2) * (1.0 + y * (1.0 / 3) * (1.0 + y * 0.25 * (1.0 + y * 0.2))))
    return jnp.where(y > -0.1, series, 1.0 - jnp.exp(y))


def split_f32(x):
    high = x.astype(jnp.bfloat16)
    return high, (x - high.astype(jnp.float32)).astype(jnp.bfloat16)


def tile_scan(a, b, reverse):
    row = lax.broadcasted_iota(jnp.int32, a.shape, 1)
    step = 1
    while step < SUB:
        shift = SUB - step if reverse else step
        keep = row < SUB - step if reverse else row >= step
        a_prev = jnp.where(keep, pltpu.roll(a, shift, 1), 1.0)
        b_prev = jnp.where(keep, pltpu.roll(b, shift, 1), 0.0)
        b = b + a * b_prev
        a = a * a_prev
        step *= 2
    return a, b


def layer_kernel(
    dims,
    mix_ref, gate_ref, cw_ref, cb_ref, decay_ref, rg_ref, rb_ref, ig_ref, ib_ref,
    res_ref, gain_ref, routes_ref, wt_ref, op_hbm, eg_hbm, eu_hbm, ed_hbm,
    stream, delta_ref,
    xp, wh, wl, af, bf, ab, bb, mixed, tok, op, proj, halo, summ, ends,
    soft_ref, wg, wu, wd, hid, gath, outg, arr, back, prem, zrec, pin, pbuf,
    op_sem, own_sem, halo_send, halo_recv, sum_send, sum_recv,
    mix_send, mix_recv, w_send, w_recv, p_send, p_recv, ga_send, ga_recv, d2_send, d2_recv,
    dis_send, dis_recv, ret_send, ret_recv, pd_send, pd_recv, zs_send, zs_recv,
    pin_send, pin_recv,
):
    S, T, L, Z = dims
    seq, C = mix_ref.shape
    rows, D = res_ref.shape
    two_cap = arr.shape[2]
    slots = S * two_cap
    heads, hd = rg_ref.shape[1], rg_ref.shape[2]
    F = eg_hbm.shape[2]
    sp = lax.axis_index("sp")
    tp = lax.axis_index("tp")
    z = lax.div(tp, 2)
    g = lax.rem(tp, 2)
    local = 2 * (1 - lax.rem(z, 2)) + g if L > 1 else 0
    upward = z < Z // 2
    inward = jnp.where(upward, z + 1, z - 1)
    middle = (z > 0) & (z < Z - 1) & (L > 1)
    cap = two_cap // 2
    top = routes_ref.shape[0]
    pair_width = 2 * F if L > 1 else F
    partner = tp + 1 - 2 * g

    op_copy = pltpu.make_async_copy(op_hbm, op, op_sem)
    op_copy.start()

    barrier = pltpu.get_barrier_semaphore()
    greeted = 0
    for ds in range(S):
        for dt in range(T):
            if (ds == 0) != (dt == 0):
                pl.semaphore_signal(
                    barrier, inc=1,
                    device_id=(lax.rem(sp + ds, S), lax.rem(tp + dt, T)),
                    device_id_type=MESH,
                )
                greeted += 1

    def remote(src, dst, send, recv, sp_to, tp_to):
        return pltpu.make_async_remote_copy(
            src_ref=src, dst_ref=dst, send_sem=send, recv_sem=recv,
            device_id=(sp_to, tp_to), device_id_type=MESH,
        )

    to_next = remote(mix_ref.at[pl.ds(seq - HALO, HALO)], halo.at[0], halo_send.at[0],
                     halo_recv.at[0], lax.rem(sp + 1, S), tp)
    to_prev = remote(mix_ref.at[pl.ds(0, HALO)], halo.at[1], halo_send.at[1],
                     halo_recv.at[1], lax.rem(sp + S - 1, S), tp)

    tensors = ((eg_hbm, wg, 1), (eu_hbm, wu, 1), (ed_hbm, wd, 0))
    depth = eg_hbm.shape[1]
    pieces = (
        (eg_hbm, wg, 1, 0, depth), (eu_hbm, wu, 1, 0, depth // 2),
        (eu_hbm, wu, 1, depth // 2, depth // 2), (ed_hbm, wd, 0, 0, F),
    )

    def chunk(ref, axis, place):
        if ref.shape[axis] == F:
            return ref
        start = pl.multiple_of(place * F, F)
        return ref.at[:, pl.ds(start, F)] if axis else ref.at[pl.ds(start, F), :]

    def weight_copy(i, core):
        src, dst, axis, first, count = pieces[i]
        side = jnp.where(upward, 0, 1)
        at = pl.ds(first, count)
        return remote(src.at[2 * lax.rem(z, 2) + core].at[at],
                      chunk(dst, axis, 2 + 2 * side + g).at[at],
                      w_send.at[i, core], w_recv.at[i, 2 * side + g], sp, 2 * inward + core)

    def partner_copy(i):
        src, dst, axis = tensors[i]
        return remote(src.at[local + 1 - 2 * g], chunk(dst, axis, g), p_send.at[i],
                      p_recv.at[i], sp, partner)

    own_weights = [
        pltpu.make_async_copy(src.at[local], chunk(dst, axis, g if L > 1 else 0), own_sem.at[i])
        for i, (src, dst, axis) in enumerate(tensors)
    ]

    def start_weights(core, which):
        if L > 1:
            for i in which:
                weight_copy(i, core).start()

    def chip_weights_arrived():
        for i in range(3):
            own_weights[i].wait()
            if L > 1:
                partner_copy(i).wait_recv()

    def weights_arrived(which):
        for i in which:
            for k in range(4):
                _, dst, axis, first, count = pieces[i]
                block = chunk(dst, axis, 2 + k).at[pl.ds(first, count)]
                pltpu.make_async_copy(block, block, w_recv.at[i, k]).wait()

    for c in own_weights:
        c.start()

    wh[...] = jnp.zeros_like(wh)
    wl[...] = jnp.zeros_like(wl)
    for k, ref in enumerate((rg_ref, ig_ref)):
        for sense in range(2):
            for h in range(heads):
                high, low = split_f32(ref[sense, h])
                col = (2 * sense + k) * C + h * hd
                wh[h * hd : (h + 1) * hd, col : col + hd] = high
                wl[h * hd : (h + 1) * hd, col : col + hd] = low
    xp[SUB : SUB + seq, :] = mix_ref[...].astype(jnp.float32)
    soft_ref[...] = jax.nn.softplus(-decay_ref[...])
    pl.semaphore_wait(barrier, greeted)
    to_next.start()
    to_prev.start()
    start_weights(0, (0, 1))
    if L > 1:
        for i in range(3):
            partner_copy(i).start()

    R = min(128, seq)

    def gates(n, _):
        base = pl.multiple_of(n * R, R)
        window = xp[pl.ds(base, R + 2 * SUB), :]
        conv = cb_ref[...] + window[SUB - 2 : SUB - 2 + R] * cw_ref[0:1]
        for tap in range(1, cw_ref.shape[0]):
            conv = conv + window[SUB - 2 + tap : SUB - 2 + tap + R] * cw_ref[tap : tap + 1]
        high, low = split_f32(conv)
        for sense, (a_ref, b_ref) in enumerate(((af, bf), (ab, bb))):
            cols = slice(2 * sense * C, (2 * sense + 2) * C)
            pre = jnp.dot(high, wh[:, cols], preferred_element_type=jnp.float32)
            pre = pre + jnp.dot(low, wh[:, cols], preferred_element_type=jnp.float32)
            pre = pre + jnp.dot(high, wl[:, cols], preferred_element_type=jnp.float32)
            recur = jax.nn.sigmoid(pre[:, :C] + rb_ref[sense : sense + 1])
            inp = jax.nn.sigmoid(pre[:, C:] + ib_ref[sense : sense + 1])
            log_a = -8.0 * recur * soft_ref[sense : sense + 1]
            a = jnp.exp(log_a)
            b = jnp.sqrt(one_minus_exp(2.0 * log_a)) * (inp * conv)
            a, b = tile_scan(
                a.reshape(R // SUB, SUB, C), b.reshape(R // SUB, SUB, C), sense == 1
            )
            a_ref[pl.ds(base, R), :] = a.reshape(R, C)
            b_ref[pl.ds(base, R), :] = b.reshape(R, C)
        return 0

    lax.fori_loop(1, seq // R - 1, gates, 0)
    to_next.wait()
    to_prev.wait()
    tail = halo[0].astype(jnp.float32)[HALO - SUB : HALO]
    head = halo[1].astype(jnp.float32)[0:SUB]
    xp[0:SUB, :] = jnp.where(sp > 0, tail, 0.0)
    xp[SUB + seq : 2 * SUB + seq, :] = jnp.where(sp < S - 1, head, 0.0)
    lax.fori_loop(0, 2, lambda n, _: gates(n * (seq // R - 1), 0), 0)

    tiles = seq // SUB

    def carry(t, held):
        sf, pf, sb, pb = held
        at = pl.ds(pl.multiple_of(t * SUB, SUB), SUB)
        a = af[at, :]
        s = bf[at, :] + a * sf
        p = a * pf
        af[at, :] = p
        bf[at, :] = s
        back = pl.ds(pl.multiple_of((tiles - 1 - t) * SUB, SUB), SUB)
        a = ab[back, :]
        s2 = bb[back, :] + a * sb
        p2 = a * pb
        ab[back, :] = p2
        bb[back, :] = s2
        return s[SUB - 1 : SUB], p[SUB - 1 : SUB], s2[0:1], p2[0:1]

    zero, one = jnp.zeros((1, C), jnp.float32), jnp.ones((1, C), jnp.float32)
    sf, pf, sb, pb = lax.fori_loop(0, tiles, carry, (zero, one, zero, one), unroll=4)
    summ[0:1, :] = sf
    summ[1:2, :] = pf
    summ[2:3, :] = sb
    summ[3:4, :] = pb
    sums = [
        remote(summ, ends.at[ds - 1], sum_send.at[ds - 1], sum_recv.at[ds - 1],
               lax.rem(sp + ds, S), tp)
        for ds in range(1, S)
    ]
    for c in sums:
        c.start()
    for c in sums:
        c.wait()
    fe, be = zero, zero
    for ds in range(S - 1, 0, -1):
        fe = jnp.where(sp >= ds, ends[ds - 1, 1:2, :] * fe + ends[ds - 1, 0:1, :], fe)
    for ds in range(1, S):
        be = jnp.where(sp + S - ds < S, ends[ds - 1, 3:4, :] * be + ends[ds - 1, 2:3, :], be)

    def join(n, _):
        at = pl.ds(pl.multiple_of(n * R, R), R)
        state = (bf[at, :] + af[at, :] * fe) + (bb[at, :] + ab[at, :] * be)
        mixed[at, :] = (state * jax.nn.gelu(gate_ref[at, :].astype(jnp.float32))).astype(
            jnp.bfloat16
        )
        return 0

    lax.fori_loop(0, seq // R, join, 0)

    def block_rows(place):
        return mixed.at[pl.ds(pl.multiple_of(place * rows, rows), rows), :]

    columns = pl.ds(pl.multiple_of(tp * C, C), C)
    moves = []
    for dt in range(1, T):
        to = lax.rem(tp + dt, T)
        moves.append(remote(block_rows(to), tok.at[:, columns], mix_send.at[dt],
                            mix_recv.at[dt], sp, to))
    for c in moves:
        c.start()
    own_move = pltpu.make_async_copy(block_rows(tp), tok.at[:, columns], own_sem.at[6])
    own_move.start()
    start_weights(0, (2,))
    op_copy.wait()
    own_move.wait()
    for c in moves:
        c.wait()

    def project(n, _):
        cols = pl.ds(pl.multiple_of(n * 256, 256), 256)
        proj[:, cols] = (
            jnp.dot(tok[...], op[:, cols], preferred_element_type=jnp.float32)
            .astype(jnp.bfloat16)
        )
        return 0

    lax.fori_loop(0, D // 256, project, 0)
    part = 32

    def norms(n, _):
        at = pl.ds(pl.multiple_of(n * part, part), part)
        s = (
            res_ref[at, :].astype(jnp.float32) + norm_rows(proj[at, :], gain_ref[0:1, :])
        ).astype(jnp.bfloat16)
        stream[at, :] = s
        gath[tp, at, :] = norm_rows(s, gain_ref[1:2, :]).astype(jnp.bfloat16)
        return 0

    lax.fori_loop(0, rows // part, norms, 0)
    wide = min(256, D)

    def chip_at(j):
        low = jnp.minimum(z, Z - 1 - z)
        d = lax.div(j + 1, 2)
        near = jnp.where(lax.rem(j, 2) == 1, z - d, z + d)
        far = jnp.where(z < Z - 1 - z, j, Z - 1 - j)
        return jnp.where(j <= 2 * low, near, far)

    def along(zc, way):
        block = gath.at[2 * zc + g]
        return remote(block, block, ga_send.at[way, zc], ga_recv.at[zc], sp, tp + 2 - 4 * way)

    def across(zc):
        block = gath.at[2 * zc + g]
        return remote(block, block, d2_send.at[zc], d2_recv.at[zc], sp, partner)

    ring = outg.shape[0]

    def dispatch(j, ds):
        zc = chip_at(j)
        to = lax.rem(sp + ds, S)
        return remote(outg.at[lax.rem(j, ring), to], arr.at[zc, sp], dis_send.at[zc, ds - 1],
                      dis_recv.at[zc, ds - 1], to, tp)

    def give_back(zc, ds):
        to = lax.rem(sp + ds, S)
        return remote(arr.at[zc, to], back.at[zc, sp], ret_send.at[zc, ds - 1],
                      ret_recv.at[zc, ds - 1], to, tp)

    def merge(zc):
        return remote(gath.at[2 * zc + 1 - g], prem.at[zc], pd_send.at[zc], pd_recv.at[zc],
                      sp, partner)

    def half_at(h):
        return pl.ds(h * (rows // 2), rows // 2)

    def deliver(zc, h):
        at = half_at(h)
        return remote(gath.at[2 * zc + g, at], zrec.at[z, at], zs_send.at[zc, h],
                      zs_recv.at[z, h], sp, 2 * zc + g)

    def slot_table(zc, weighted):
        at = pl.ds(pl.multiple_of(zc * (2 * rows), 2 * rows), 2 * rows)
        named, given = routes_ref[:, at], wt_ref[:, at]
        high_rows = max(16, S)
        experts = lax.broadcasted_iota(jnp.int32, (high_rows, 2 * rows), 0) * L + local
        hit = experts == named[0:1]
        share = jnp.where(hit, given[0:1], 0.0)
        for k in range(1, top):
            same = experts == named[k : k + 1]
            hit = hit | same
            share = jnp.where(same, given[k : k + 1], share)
        earlier = lax.broadcasted_iota(jnp.int32, (2 * rows, 2 * rows), 0)
        token = lax.broadcasted_iota(jnp.int32, (2 * rows, 2 * rows), 1)
        inside = jnp.where(token >= rows, rows, 0)
        before = jnp.where((earlier < token) & (earlier >= inside), 1.0, 0.0)
        rank = jnp.dot(
            jnp.where(hit, 1.0, 0.0).astype(jnp.bfloat16), before.astype(jnp.bfloat16),
            preferred_element_type=jnp.float32,
        ).astype(jnp.int32)
        column = lax.broadcasted_iota(jnp.int32, (high_rows, 2 * rows), 1)
        place = jnp.where(hit, rank + jnp.where(column >= rows, cap, 0), -1)
        slot_id = lax.broadcasted_iota(jnp.int32, (two_cap, 2 * rows), 0)
        pieces = [
            jnp.where(slot_id == place[s : s + 1], share[s : s + 1] if weighted else 1.0, 0.0)
            for s in range(S)
        ]
        return jnp.concatenate(pieces, axis=0)

    def gather_step(j):
        zc = chip_at(j)

        @pl.when(j > 0)
        def _():
            pltpu.make_async_copy(gath.at[2 * zc + g], gath.at[2 * zc + g], ga_recv.at[zc]).wait()

        across(zc).start()

        @pl.when((zc <= z) & (z < Z - 1))
        def _():
            along(zc, 0).start()

        @pl.when((zc >= z) & (z > 0))
        def _():
            along(zc, 1).start()

        @pl.when(zc == jnp.where(upward, 0, Z - 1))
        def _():
            start_weights(0, (3,))
            start_weights(1, (0, 1, 2, 3))

        across(zc).wait_recv()
        selector = slot_table(zc, False).astype(jnp.bfloat16)
        slot = lax.rem(j, ring)

        @pl.when(j >= ring)
        def _():
            for ds in range(1, S):
                dispatch(j - ring, ds).wait_send()

        def pick(n, _):
            cols = pl.ds(pl.multiple_of(n * wide, wide), wide)
            tokens = gath[pl.ds(2 * zc, 2), :, cols].reshape(2 * rows, wide)
            picked = jnp.dot(selector, tokens, preferred_element_type=jnp.float32)
            outg[slot, :, :, cols] = picked.astype(jnp.bfloat16).reshape(S, two_cap, wide)
            return 0

        lax.fori_loop(0, D // wide, pick, 0)
        for ds in range(1, S):
            dispatch(j, ds).start()
        arr[zc, sp] = outg[slot, sp]

    def activate(x, gate_w, up_w):
        gate_act = jnp.dot(x, gate_w, preferred_element_type=jnp.float32)
        up_act = jnp.dot(x, up_w, preferred_element_type=jnp.float32)
        return (jax.nn.silu(gate_act) * up_act).astype(jnp.bfloat16)

    def up_part(j, n):
        zc = chip_at(j)
        cols = pl.ds(pl.multiple_of(n * pair_width, pair_width), pair_width)
        if L == 1:
            cols = slice(None)
        hid[zc, :, cols] = activate(arr[zc].reshape(slots, D), wg[:, cols], wu[:, cols])

    def down_part(zc, depth):
        def down(n, _):
            cols = pl.ds(pl.multiple_of(n * wide, wide), wide)
            rows_out = jnp.dot(
                hid[zc, :, :depth], wd[:depth, cols], preferred_element_type=jnp.float32
            )
            arr[zc, :, :, cols] = rows_out.astype(jnp.bfloat16).reshape(S, two_cap, wide)
            return 0

        lax.fori_loop(0, D // wide, down, 0)

    def return_rows(zc):
        for ds in range(1, S):
            give_back(zc, ds).start()

    early = middle & (g == 0)
    pair_chip = z + 1 - 2 * lax.rem(z, 2)

    def return_order(i):
        pair_at = jnp.where((lax.rem(z, 2) == 1) | (z == 0), 1, 2)
        others = jnp.where(i + 1 < pair_at, i + 1, i + 2)
        ordered = jnp.where(i < Z - 2, others, jnp.where(i == Z - 2, pair_at, 0))
        return chip_at(jnp.where(middle, lax.rem(i + 1, Z), ordered))

    def stage(j, _):
        @pl.when(j < Z)
        def _():
            gather_step(j)

        @pl.when(j == 1)
        def _():
            chip_weights_arrived()
            if L > 1:

                @pl.when(early)
                def _():
                    weights_arrived((0, 1, 2))

        @pl.when(j > 0)
        def _():
            for ds in range(1, S):
                dispatch(j - 1, ds).wait_recv()

            def part_of(n, _):
                up_part(j - 1, n)
                return 0

            lax.fori_loop(0, jnp.where(early, 3, 1), part_of, 0)

            @pl.when(jnp.logical_not(middle))
            def _():
                down_part(chip_at(j - 1), pair_width)

                @pl.when((j > 1) & (chip_at(j - 1) != pair_chip))
                def _():
                    return_rows(chip_at(j - 1))

        return 0

    lax.fori_loop(0, Z + 1, stage, 0)

    @pl.when(jnp.logical_not(middle))
    def _():
        return_rows(pair_chip)
        return_rows(z)

    if L > 1:

        @pl.when(middle)
        def _():
            @pl.when(g == 1)
            def _():
                weights_arrived((0, 1, 2))

                def rest(n, _):
                    up_part(lax.div(n, 2), 1 + lax.rem(n, 2))
                    return 0

                lax.fori_loop(0, 2 * Z, rest, 0)

            weights_arrived((3,))

            def finish_rows(i, _):
                down_part(return_order(i), 3 * pair_width)
                return_rows(return_order(i))
                return 0

            lax.fori_loop(0, Z, finish_rows, 0)


    def feeds(zc):
        return (zc != z) & (zc != pair_chip) & ((zc > z) == (lax.rem(z, 2) == 0))

    def relays(zc):
        return (zc != z) & (zc != pair_chip) & ((zc > z) != (lax.rem(z, 2) == 0))

    def feed(zc, h):
        at = half_at(h)
        return remote(gath.at[2 * zc + g, at], pin.at[zc, at], pin_send.at[zc, h],
                      pin_recv.at[zc, h], sp, 2 * pair_chip + g)

    def combine(i, _):
        zc = return_order(i)
        across(zc).wait_send()

        @pl.when((zc <= z) & (z < Z - 1))
        def _():
            along(zc, 0).wait_send()

        @pl.when((zc >= z) & (z > 0))
        def _():
            along(zc, 1).wait_send()

        table = jnp.transpose(slot_table(zc, True))
        high, low = split_f32(table)
        for ds in range(1, S):
            give_back(zc, ds).wait_recv()
        back[zc, sp] = arr[zc, sp]

        def mix(n, _):
            cols = pl.ds(pl.multiple_of(n * wide, wide), wide)
            values = back[zc, :, :, cols].reshape(slots, wide)
            total = jnp.dot(high, values, preferred_element_type=jnp.float32)
            total = total + jnp.dot(low, values, preferred_element_type=jnp.float32)
            pbuf[:, :, cols] = total.reshape(2, rows, wide)
            return 0

        lax.fori_loop(0, D // wide, mix, 0)
        gath[2 * zc + 1 - g] = pbuf[1 - g].astype(jnp.bfloat16)
        merge(zc).start()
        merge(zc).wait_recv()

        for h in range(2):
            at = half_at(h)

            @pl.when(relays(zc))
            def _():
                pltpu.make_async_copy(pin.at[zc, at], pin.at[zc, at], pin_recv.at[zc, h]).wait()
                gath[2 * zc + g, at] = (
                    pbuf[g, at] + prem[zc, at].astype(jnp.float32)
                    + pin[zc, at].astype(jnp.float32)
                ).astype(jnp.bfloat16)

            @pl.when(feeds(zc) | (zc == pair_chip))
            def _():
                gath[2 * zc + g, at] = (
                    pbuf[g, at] + prem[zc, at].astype(jnp.float32)
                ).astype(jnp.bfloat16)

            @pl.when(feeds(zc))
            def _():
                feed(zc, h).start()

            @pl.when(relays(zc) | (zc == pair_chip))
            def _():
                deliver(zc, h).start()

        return 0

    lax.fori_loop(0, Z, combine, 0)

    senders = [pair_chip]
    for m in range(1, Z // 2):
        other = lax.rem(lax.div(z, 2) + m, Z // 2)
        senders.append(2 * other + jnp.where(2 * other < z, 1, 0))
    for zc in senders:
        for h in range(2):
            block = zrec.at[zc, half_at(h)]
            pltpu.make_async_copy(block, block, zs_recv.at[zc, h]).wait()

    def finish(n, _):
        at = pl.ds(pl.multiple_of(n * part, part), part)
        total = pbuf[g, at, :] + prem[z, at, :].astype(jnp.float32)
        for zc in senders:
            total = total + zrec[zc, at, :].astype(jnp.float32)
        mixture = total.astype(jnp.bfloat16)
        delta_ref[at, :] = norm_rows(mixture, gain_ref[2:3, :])
        return 0

    lax.fori_loop(0, rows // part, finish, 0)
    if L > 1:
        for i in range(3):
            partner_copy(i).wait_send()
        for i in range(4):
            for core in range(2):
                weight_copy(i, core).wait_send()
    for j in range(max(0, Z - ring), Z):
        for ds in range(1, S):
            dispatch(j, ds).wait_send()
    for zc in range(Z):
        for ds in range(1, S):
            give_back(zc, ds).wait_send()
        merge(zc).wait_send()

    def drain(i, _):
        zc = return_order(i)

        @pl.when(feeds(zc))
        def _():
            for h in range(2):
                feed(zc, h).wait_send()

        @pl.when((zc != z) & jnp.logical_not(feeds(zc)))
        def _():
            for h in range(2):
                deliver(zc, h).wait_send()

        return 0

    lax.fori_loop(0, Z, drain, 0)


def on_device(
    mix_in, gate_in, conv_w, conv_b, decay_param, recur_gate, recur_bias, input_gate, input_bias,
    residual, out_proj, norm_gain, routes, route_wt, exp_gate, exp_up, exp_down,
):
    S, T = lax.axis_size("sp"), lax.axis_size("tp")
    L, D, F = exp_gate.shape
    Z = T // 2
    dims = (S, T, L, Z)
    seq, C = mix_in.shape
    rows = residual.shape[0]
    cap = 2 * rows * routes.shape[1] // (L * S)
    vmem = pl.BlockSpec(memory_space=pltpu.VMEM)
    hbm = pl.BlockSpec(memory_space=pltpu.MemorySpace.HBM)
    b16, f32 = jnp.bfloat16, jnp.float32
    dma = pltpu.SemaphoreType.DMA
    hidden = 6 * F if L > 1 else F
    up_shape = (D, hidden)
    stream, delta = pl.pallas_call(
        functools.partial(layer_kernel, dims),
        out_shape=(jax.ShapeDtypeStruct((rows, D), b16), jax.ShapeDtypeStruct((rows, D), f32)),
        in_specs=[vmem] * 13 + [hbm] * 4,
        out_specs=(vmem, vmem),
        scratch_shapes=[
            pltpu.VMEM((seq + 2 * SUB, C), f32),
            pltpu.VMEM((C, 4 * C), b16),
            pltpu.VMEM((C, 4 * C), b16),
            pltpu.VMEM((seq, C), f32), pltpu.VMEM((seq, C), f32),
            pltpu.VMEM((seq, C), f32), pltpu.VMEM((seq, C), f32),
            pltpu.VMEM((seq, C), b16),
            pltpu.VMEM((rows, T * C), b16),
            pltpu.VMEM(out_proj.shape, b16),
            pltpu.VMEM((rows, D), b16),
            pltpu.VMEM((2, HALO, C), b16),
            pltpu.VMEM((SUB, C), f32),
            pltpu.VMEM((S - 1, SUB, C), f32),
            pltpu.VMEM((2, C), f32),
            pltpu.VMEM(up_shape, b16), pltpu.VMEM(up_shape, b16), pltpu.VMEM((hidden, D), b16),
            pltpu.VMEM((Z, S * 2 * cap, hidden), b16),
            pltpu.VMEM((T, rows, D), b16),
            pltpu.VMEM((min(Z, RING), S, 2 * cap, D), b16),
            pltpu.VMEM((Z, S, 2 * cap, D), b16),
            pltpu.VMEM((Z, S, 2 * cap, D), b16),
            pltpu.VMEM((Z, rows, D), b16),
            pltpu.VMEM((Z, rows, D), b16),
            pltpu.VMEM((Z, rows, D), b16),
            pltpu.VMEM((2, rows, D), f32),
            dma, dma((8,)),
            dma((2,)), dma((2,)),
            dma((S - 1,)), dma((S - 1,)),
            dma((T,)), dma((T,)),
            dma((4, 2)), dma((4, 4)),
            dma((3,)), dma((3,)),
            dma((2, Z)), dma((Z,)),
            dma((Z,)), dma((Z,)),
            dma((Z, S - 1)), dma((Z, S - 1)),
            dma((Z, S - 1)), dma((Z, S - 1)),
            dma((Z,)), dma((Z,)),
            dma((Z, 2)), dma((Z, 2)),
            dma((Z, 2)), dma((Z, 2)),
        ],
        compiler_params=pltpu.CompilerParams(
            collective_id=0, has_side_effects=True, vmem_limit_bytes=63 * 1024 * 1024
        ),
    )(
        mix_in, gate_in, conv_w, conv_b.reshape(1, C), decay_param, recur_gate, recur_bias,
        input_gate, input_bias, residual, norm_gain, routes.T, route_wt.T, out_proj,
        exp_gate, exp_up, exp_down,
    )
    return (stream.astype(f32) + delta).astype(b16)


def solution(mesh):
    return jax.shard_map(
        on_device,
        mesh=mesh,
        in_specs=(
            P("sp", "tp"),
            P("sp", "tp"),
            P(None, "tp"),
            P("tp"),
            P(None, "tp"),
            P(None, "tp", None, None),
            P(None, "tp"),
            P(None, "tp", None, None),
            P(None, "tp"),
            P(("sp", "tp"), None),
            P(),
            P(),
            P("sp", None),
            P("sp", None),
            P("sp", None, "tp"),
            P("sp", None, "tp"),
            P("sp", "tp", None),
        ),
        out_specs=P(("sp", "tp"), None),
        check_vma=False,
    )
```
